256 devices in a mesh: ra: 32 (over z, y), cb: 8 (over x, core).
Axes of the slice: x: 4, y: 4, z: 8, core: 2. Of those that a mesh axis runs over, the one named last changes fastest.
Arguments:
- tokens: bfloat16 [2048, 16384], P('ra'), may hold values from -16 to 16
- norm_gain: float32 [2, 2048], replicated, may hold values from 0.1 to 1.9
- up_weight: float32 [2, 2048, 6144], P(None, 'ra', 'cb'), may hold values from -0.125 to 0.125
- gate_weight: float32 [2, 2048, 6144], P(None, 'ra', 'cb'), may hold values from -0.125 to 0.125
- up_scale: float32 [2, 6144], P(None, 'cb'), may hold values from 0.5 to 2
- gate_scale: float32 [2, 6144], P(None, 'cb'), may hold values from 0.5 to 2
- up_taps: float32 [2, 3, 6144], P(None, None, 'cb'), may hold values from -3 to 3
- gate_taps: float32 [2, 3, 6144], P(None, None, 'cb'), may hold values from -3 to 3
- down_weight: float32 [2, 2048, 6144], P(None, 'ra', 'cb'), may hold values from -0.078125 to 0.078125
- down_scale: float32 [2, 2048], replicated, may hold values from 0.5 to 2
Outputs:
- mixed: bfloat16 [2048, 16384], P('ra')
The draws below stay inside these ranges and needn't reach their ends.
All inputs are finite; a program needn't handle non-finite values.
Results may differ from the reference program's by a relative error of at most 0.024.
Values may be sent and summed in bfloat16 or wider, within the bound.
A program may use at most 64 MiB of HBM per device.

```python
import math
import jax
import jax.numpy as jnp
from jax import lax

D = 2048
FF = 6144
KW = 3
LAYERS = 2
TOKENS = 16384
N_RA = 32
N_CB = 8


def draw_tokens(key, part):
    first, second, third = jax.random.split(key, 3)
    blocks = jnp.exp(jax.random.uniform(second, (N_RA,), jnp.float32, math.log(0.3), math.log(3.0)))
    features = jnp.repeat(blocks, D // N_RA, total_repeat_length=D)
    base = jnp.clip(jax.random.normal(first, (D, TOKENS), jnp.float32), -4.0, 4.0)
    return (base * features[:, None]).astype(jnp.bfloat16)


def shard_levels(rng, extent, cuts, smallest, high):
    gain, own = 1.0, jax.random.fold_in(rng, 6)
    for position, parts in cuts:
        draws = jnp.exp(jax.random.uniform(jax.random.fold_in(own, position), (parts,), jnp.float32, smallest / len(cuts), high / len(cuts)))
        gain = gain * jnp.repeat(draws, extent[position] // parts).reshape([-1 if axis == position else 1 for axis in range(len(extent))])
    return gain


def normal_values(stream_key, extent, scale, bound, pieces=(), dtype=jnp.bfloat16):
    level = shard_levels(stream_key, extent, pieces, -0.22, 0.18) if pieces else 1.0
    values = jax.random.normal(stream_key, extent, jnp.float32) * scale * level
    return jnp.minimum(jnp.maximum(values, -bound), bound).astype(dtype)


def setup_inputs(seed: int = 0) -> dict:
    splits = jax.random.split(jax.random.key(seed), 11)
    return {
        "tokens": draw_tokens(jax.random.fold_in(splits[10], 71), 0),
        "norm_gain": jnp.clip(1.0 + 0.18 * jax.random.normal(splits[1], (LAYERS, D), jnp.float32), 0.1, 1.9),
        "up_weight": normal_values(splits[2], (LAYERS, D, FF), D ** -0.5, 0.125, ((1, 32), (2, 8)), jnp.float32),
        "gate_weight": normal_values(splits[3], (LAYERS, D, FF), D ** -0.5, 0.125, ((1, 32), (2, 8)), jnp.float32),
        "up_scale": jnp.clip(jnp.exp(math.log(2.0) - 1.3862944 * jax.random.uniform(splits[4], (LAYERS, FF), jnp.float32) ** shard_levels(splits[4], (LAYERS, FF), ((1, 8),), -0.2, 0.2)), 0.5, 2.0),
        "gate_scale": jnp.clip(jnp.exp(math.log(2.0) - 1.3862944 * jax.random.uniform(splits[5], (LAYERS, FF), jnp.float32) ** shard_levels(splits[5], (LAYERS, FF), ((1, 8),), -0.2, 0.2)), 0.5, 2.0),
        "up_taps": normal_values(splits[6], (LAYERS, KW, FF), 0.6, 3.0, ((2, 8),), jnp.float32),
        "gate_taps": normal_values(splits[7], (LAYERS, KW, FF), 0.6, 3.0, ((2, 8),), jnp.float32),
        "down_weight": normal_values(splits[8], (LAYERS, D, FF), FF ** -0.5, 0.078125, ((1, 32), (2, 8)), jnp.float32),
        "down_scale": jnp.clip(jnp.exp(jax.random.uniform(splits[9], (LAYERS, D), jnp.float32, math.log(0.5), math.log(2.0))), 0.5, 2.0),
    }


EPS = 1e-06
RESIDUAL = 0.5

def causal_taps(values, taps):
    width = taps.shape[0]
    length = values.shape[0]
    padded = jnp.pad(values, ((width - 1, 0), (0, 0)))
    total = jnp.zeros_like(values)
    for k in range(width):
        total = total + taps[k][None, :] * padded[k:k + length]
    return total

def reference(tokens, norm_gain, up_weight, gate_weight, up_scale, gate_scale, up_taps, gate_taps, down_weight, down_scale):
    state = tokens.T
    block = FF // N_CB
    for layer in range(LAYERS):
        state_f = state.astype(jnp.float32)
        inverse = lax.rsqrt(lax.optimization_barrier(jnp.mean(state_f * state_f, axis=1, keepdims=True)) + EPS)
        scaled = (state_f * norm_gain[layer][None, :]).astype(jnp.bfloat16)
        up_raw = jnp.dot(scaled, up_weight[layer].astype(jnp.bfloat16), preferred_element_type=jnp.float32)
        gate_raw = jnp.dot(scaled, gate_weight[layer].astype(jnp.bfloat16), preferred_element_type=jnp.float32)
        up_pre = up_raw * inverse * up_scale[layer][None, :]
        gate_pre = gate_raw * inverse * gate_scale[layer][None, :]
        conv_up = causal_taps(up_pre, up_taps[layer])
        conv_gate = causal_taps(gate_pre, gate_taps[layer])
        hidden = (jax.nn.silu(conv_gate) * conv_up).astype(jnp.bfloat16)
        weight_b = down_weight[layer].astype(jnp.bfloat16)
        down = jnp.zeros((hidden.shape[0], weight_b.shape[0]), jnp.float32)
        for group in range(N_CB):
            term = jnp.dot(hidden[:, group * block:(group + 1) * block], weight_b[:, group * block:(group + 1) * block].T, preferred_element_type=jnp.float32)
            rounded = lax.optimization_barrier(term.astype(jnp.bfloat16))
            down = down + rounded.astype(jnp.float32)
        state = (down * down_scale[layer][None, :] + RESIDUAL * state_f).astype(jnp.bfloat16)
    return state.T
```

```python
import jax
import jax.numpy as jnp
from jax import lax
from jax.experimental import pallas as pl
from jax.experimental.pallas import tpu as pltpu
from jax.sharding import Mesh
from jax.sharding import PartitionSpec as P

MESH = pl.DeviceIdType.MESH
EPS = 1e-06
RESIDUAL = 0.5
NZ, NY, NX = 8, 4, 4
NR = NZ * NY
CHUNKS = 2

ITEMS = [(m, 0, (256, 384, 256)[m % 3], 768) for m in range(6)]
GATHER_KEYS = ("Ay1", "Ay2", "Az1", "Az2", "Az3", "Az4", "Bz1", "Bz2", "Bz3", "Bz4", "By1", "By2")
KEY = {k + d: i for i, (k, d) in enumerate([(k, d) for k in GATHER_KEYS for d in "pm"])}
SHARE_KEYS = {k: i for i, k in enumerate(("X1p", "X1m", "X2p", "X2m", "D0", "D1", "D2", "D3"))}
SUM_KEYS = {k: i for i, k in enumerate(("D", "Ap", "Am", "Bp", "Bm"))}


def default_order():
    gather = []
    for i in range(len(ITEMS)):
        for st in range(7):
            gather.append((i + st, i, st))
    gather.sort()
    slots = [[(ph, i, st) for t, i, st in gather if t == s for ph in "AB"] for s in range(len(ITEMS) + 6)]
    chunks = range(CHUNKS)

    def share(which, st):
        return [("share", which, j, st) for j in chunks]

    def layer(l):
        ug = [("prep", l)]
        for n in range(3):
            ug += [("ug", l, n), ("halo", l, n)]
        dn = [("conv", l)]
        for j in chunks:
            dn += [("down", l, j), ("sum", l, j, 0)]
        return ug, dn

    after = {s: [] for s in range(len(slots))}
    after[0] = [("in", 0)]
    after[2] = [("in", 1)] + share(0, 0)
    after[3] = share(0, 1)
    after[4] = share(0, 2)
    after[5] = share(0, 3)
    ug, dn = layer(0)
    after[7] = ug
    after[8] = dn + [("sum", 0, j, 1) for j in chunks] + [("sum", 0, j, 2) for j in chunks]
    after[9] = [("sum", 0, j, 3) for j in chunks] + share(1, 0) + share(1, 1)
    after[10] = share(1, 2) + share(1, 3)
    ug, dn = layer(1)
    order = []
    for s, slot in enumerate(slots):
        if s == len(slots) - 1:
            order += ug
        order += slot + after[s]
    order += dn
    for st in (1, 2, 3):
        order += [("sum", 1, j, st) for j in chunks]
    order += [("out", 0)]
    for st in range(4):
        order += share(2, st)
    return order


ORDER = default_order()


class Program:
    def __init__(self, refs):
        (
            self.tok, self.w_in, self.gain, self.us, self.gs, self.ut, self.gt, self.ds, self.out,
            self.w, self.s, self.x, self.pre, self.halo, self.hid, self.part, self.rd, self.q,
            self.rh, self.rf, self.fin,
            self.l_sem, self.gs_sem, self.gr_sem, self.is_sem, self.ir_sem, self.ss_sem, self.sr_sem,
            self.us_sem, self.ur_sem, self.hs_sem, self.hr_sem, self.os_sem, self.or_sem,
        ) = refs
        self.zi, self.yi = lax.axis_index("z"), lax.axis_index("y")
        self.xi, self.ci = lax.axis_index("x"), lax.axis_index("c")
        self.ri = self.zi * NY + self.yi
        self.span = NR // CHUNKS
        self.loaded = set()
        self.w_copies = [
            pltpu.make_async_copy(self.w_in.at[m], self.w.at[m, self.zi, self.yi], self.l_sem.at[m])
            for m in range(6)
        ]

    def gather_region(self, i, key, d, recv):
        m, c0, c1, c2 = ITEMS[i]
        sign = 1 if d == "p" else -1
        hop = int(key[2])
        back = hop if recv else hop - 1
        first, second = pl.ds(c0, c1 - c0), pl.ds(c1, c2 - c1)
        z = lax.rem(self.zi - sign * back + NZ, NZ)
        y = lax.rem(self.yi - sign * back + NY, NY)
        half = pl.ds(0 if d == "p" else 32, 32)
        w = self.w.at[m]
        if key[:2] == "Ay":
            return w.at[self.zi, y, half if hop == 2 else slice(None), first]
        if key[:2] == "Az":
            if hop == 4:
                return w.at[z, pl.ds(0 if d == "p" else 2, 2), :, first]
            return w.at[z, :, :, first]
        if key[:2] == "Bz":
            return w.at[z, self.yi, half if hop == 4 else slice(None), second]
        if hop == 2:
            return w.at[pl.ds(0 if d == "p" else 4, 4), y, :, second]
        return w.at[:, y, :, second]

    def step_to(self, link, d):
        if link == "z":
            return {"z": lax.rem(self.zi + (1 if d == "p" else NZ - 1), NZ)}
        if link == "y":
            return {"y": lax.rem(self.yi + (1 if d == "p" else NY - 1), NY)}
        if link == "x":
            return {"x": lax.rem(self.xi + (1 if d == "p" else NX - 1), NX)}
        return {"c": 1 - self.ci}

    @staticmethod
    def remote(src, dst, send, recv, to):
        return pltpu.make_async_remote_copy(
            src_ref=src, dst_ref=dst, send_sem=send, recv_sem=recv, device_id=to, device_id_type=MESH
        )

    def g_copy(self, i, key, d, recv=False):
        region = self.gather_region(i, key, d, recv)
        k = KEY[key + d]
        return self.remote(
            region, region, self.gs_sem.at[i, k], self.gr_sem.at[i, k], self.step_to(key[1], d)
        )

    def g_send(self, i, key):
        for d in "pm":
            self.g_copy(i, key, d).start()

    def g_wait(self, i, key):
        for d in "pm":
            self.g_copy(i, key, d, True).wait_recv()

    def g_forward(self, i, came, goes):
        for d in "pm":
            self.g_copy(i, came, d, True).wait_recv()
            self.g_copy(i, goes, d).start()

    def own_weights(self, i):
        m = ITEMS[i][0]
        if m not in self.loaded:
            self.loaded.add(m)
            self.w_copies[m].wait()

    def A(self, i, st):
        self.own_weights(i)
        if st == 0:
            self.g_send(i, "Ay1")
        elif st == 1:
            self.g_forward(i, "Ay1", "Ay2")
        elif st == 2:
            self.g_wait(i, "Ay2")
            self.g_send(i, "Az1")
        elif st < 6:
            self.g_forward(i, f"Az{st - 2}", f"Az{st - 1}")
        else:
            self.g_wait(i, "Az4")

    def B(self, i, st):
        self.own_weights(i)
        if st == 0:
            self.g_send(i, "Bz1")
        elif st < 4:
            self.g_forward(i, f"Bz{st}", f"Bz{st + 1}")
        elif st == 4:
            self.g_wait(i, "Bz4")
            self.g_send(i, "By1")
        elif st == 5:
            self.g_forward(i, "By1", "By2")
        else:
            self.g_wait(i, "By2")

    def lanes(self, own=True):
        c = self.ci if own else 1 - self.ci
        return pl.ds(pl.multiple_of(c * 256, 256), 256)

    def in_own(self):
        cols = pl.ds(pl.multiple_of(self.ri * 512 + self.ci * 256, 256), 256)
        rows = pl.ds(pl.multiple_of(self.xi * 16, 16), 16)
        return pltpu.make_async_copy(
            self.tok.at[rows, cols], self.s.at[0, self.ri, self.xi, :, self.lanes()], self.l_sem.at[6]
        )

    def in_copy(self, other, recv=False):
        cols = pl.ds(pl.multiple_of(other * 512 + self.ci * 256, 256), 256)
        rows = pl.ds(pl.multiple_of(self.xi * 16, 16), 16)
        lands = other if recv else self.ri
        return self.remote(
            self.tok.at[rows, cols],
            self.s.at[0, lands, self.xi, :, self.lanes()],
            self.is_sem.at[other],
            self.ir_sem.at[lands],
            {"z": other // NY, "y": lax.rem(other, NY)},
        )

    def each_other(self, do):
        def body(k, carry):
            do(lax.rem(self.ri + k, NR))
            return carry

        lax.fori_loop(1, NR, body, 0)

    def in_(self, st):
        if st == 0:
            self.in_own().start()
            self.each_other(lambda o: self.in_copy(o).start())
        else:
            self.in_own().wait()
            self.each_other(lambda o: self.in_copy(o, True).wait_recv())

    def share_copy(self, which, j, key, recv=False):
        r = self.span
        lo, n = j * r, r
        if key[0] == "X":
            sign = 1 if key[2] == "p" else -1
            hop = int(key[1])
            back = hop if recv else hop - 1
            x = lax.rem(self.xi - sign * back + NX, NX)
            if hop == 2:
                n = r // 2
                lo += 0 if key[2] == "p" else n
            lanes, to = self.lanes(), self.step_to("x", key[2])
        else:
            off = {"D0": 0, "D1": NX - 1, "D2": 1, "D3": 2}[key]
            x = lax.rem(self.xi + off, NX)
            lanes, to = self.lanes(not recv), self.step_to("c", "p")
        region = self.s.at[which, pl.ds(lo, n), x, :, lanes]
        k = SHARE_KEYS[key]
        return self.remote(
            region, region, self.ss_sem.at[which, j, k], self.sr_sem.at[which, j, k], to
        )

    def share(self, which, j, st):
        def start(*keys):
            for k in keys:
                self.share_copy(which, j, k).start()

        def wait(*keys):
            for k in keys:
                self.share_copy(which, j, k, True).wait_recv()

        if st == 0:
            start("X1p", "X1m", "D0")
        elif st == 1:
            wait("X1p")
            start("X2p", "D1")
            wait("X1m")
            start("X2m", "D2")
        elif st == 2:
            wait("X2p", "X2m")
            start("D3")
        else:
            wait("D0", "D1", "D2", "D3")

    def prep(self, l):
        def body(k, acc):
            block = self.s[l, pl.ds(k * 4, 4)].reshape(256, 512)
            t = block.T.astype(jnp.float32)
            cols = pl.ds(pl.multiple_of(k * 256, 256), 256)
            self.x[:, cols] = (t * self.gain[l : l + 1, cols]).astype(jnp.bfloat16)
            sq = t * t
            return acc + sq[:, :128] + sq[:, 128:]

        acc = lax.fori_loop(0, 8, body, jnp.zeros((512, 128), jnp.float32))
        mean = jnp.sum(acc, axis=1, keepdims=True) * (1.0 / 2048)
        self.inverse = lax.rsqrt(mean + EPS)

    def ug(self, l, n):
        cols = slice(n * 256, n * 256 + 256)
        for k, scale in ((0, self.us), (1, self.gs)):
            w = self.w[3 * l + k, :, :, :, cols].reshape(2048, 256)
            raw = jnp.dot(self.x[...], w, preferred_element_type=jnp.float32)
            self.pre[k, 8:520, cols] = raw * self.inverse * scale[l : l + 1, cols]

    def halo_copy(self, l, n):
        cols = pl.ds(n * 256, 256)
        wrap = jnp.where(self.yi == NY - 1, 1, 0)
        to = {"z": lax.rem(self.zi + wrap, NZ), "y": lax.rem(self.yi + 1, NY)}
        return self.remote(
            self.pre.at[:, pl.ds(512, 8), cols], self.halo.at[l, :, :, cols],
            self.hs_sem.at[l, n], self.hr_sem.at[l, n], to,
        )

    def conv(self, l):
        for n in range(3):
            self.halo_copy(l, n).wait_recv()
        first = self.ri == 0
        for n in range(6):
            cols = slice(n * 128, n * 128 + 128)
            both = []
            for k, taps in ((0, self.ut), (1, self.gt)):
                before = self.halo[l, k, :, cols]
                self.pre[k, 0:8, cols] = jnp.where(first, jnp.zeros_like(before), before)
                total = taps[l, 0:1, cols] * self.pre[k, 6:518, cols]
                total += taps[l, 1:2, cols] * self.pre[k, 7:519, cols]
                total += taps[l, 2:3, cols] * self.pre[k, 8:520, cols]
                both.append(total)
            up, gate = both
            self.hid[:, cols] = (gate / (1.0 + jnp.exp(-gate)) * up).astype(jnp.bfloat16)
        for n in range(3):
            self.halo_copy(l, n).wait_send()

    def down(self, l, j):
        def body(k, carry):
            z = j * (NZ // CHUNKS) + k
            w = self.w[3 * l + 2, z].reshape(256, 768)
            part = lax.dot_general(
                w, self.hid[...], (((1,), (1,)), ((), ())), preferred_element_type=jnp.float32
            )
            self.part[l, pl.ds(z * NY, NY)] = part.astype(jnp.bfloat16).reshape(NY, 4, 16, 512)
            return carry

        lax.fori_loop(0, NZ // CHUNKS, body, 0)

    def sum_copy(self, l, j, key):
        r = self.span
        h = r // 2
        k = SUM_KEYS[key]
        sems = (self.us_sem.at[l, j, k], self.ur_sem.at[l, j, k])
        if key == "D":
            return self.remote(
                self.part.at[l, pl.ds(j * r, r), :, :, self.lanes(False)],
                self.rd.at[l, pl.ds(j * r, r)], *sems, self.step_to("c", "p"),
            )
        d = key[1]
        if key[0] == "A":
            lo = j * r + (0 if d == "p" else h)
            return self.remote(
                self.q.at[l, pl.ds(lo, h), lax.rem(self.xi + 2, NX)],
                self.rh.at[l, 0 if d == "p" else 1, pl.ds(j * h, h)], *sems, self.step_to("x", d),
            )
        return self.remote(
            self.q.at[l, pl.ds(j * r, r), lax.rem(self.xi + (1 if d == "p" else NX - 1), NX)],
            self.rf.at[l, 0 if d == "p" else 1, pl.ds(j * r, r)], *sems, self.step_to("x", d),
        )

    def sum(self, l, j, st):
        r = self.span
        h = r // 2
        f32 = jnp.float32
        rows = pl.ds(j * r, r)
        if st == 0:
            self.sum_copy(l, j, "D").start()
        elif st == 1:
            self.sum_copy(l, j, "D").wait_recv()
            mine = self.part[l, rows, :, :, self.lanes()].astype(f32)
            self.q[l, rows] = (mine + self.rd[l, rows].astype(f32)).astype(jnp.bfloat16)
            self.sum_copy(l, j, "Ap").start()
            self.sum_copy(l, j, "Am").start()
        elif st == 2:
            for d, key in ((1, "p"), (-1, "m")):
                self.sum_copy(l, j, "A" + key).wait_recv()
                x = lax.rem(self.xi + d + NX, NX)
                part = pl.ds(j * r + (0 if key == "p" else h), h)
                came = self.rh[l, 0 if key == "p" else 1, pl.ds(j * h, h)].astype(f32)
                self.q[l, part, x] = (self.q[l, part, x].astype(f32) + came).astype(jnp.bfloat16)
                self.sum_copy(l, j, "B" + key).start()
        else:
            self.sum_copy(l, j, "Bp").wait_recv()
            self.sum_copy(l, j, "Bm").wait_recv()
            total = self.q[l, rows, self.xi].astype(f32)
            total += self.rf[l, 0, rows].astype(f32) + self.rf[l, 1, rows].astype(f32)
            scale = self.ds[l, rows]
            scale = jnp.concatenate([scale, scale], axis=2)
            old = self.s[l, rows, self.xi, :, self.lanes()].astype(f32)
            new = (total * scale + RESIDUAL * old).astype(jnp.bfloat16)
            if l == 0:
                self.s[1, rows, self.xi, :, self.lanes()] = new
            else:
                self.fin[rows] = new
                self.each_in(j, lambda o: self.out_copy(o).start())

    def out_copy(self, other, recv=False):
        lands = other if recv else self.ri
        return self.remote(
            self.fin.at[other],
            self.s.at[2, lands, self.xi, :, self.lanes()],
            self.os_sem.at[other],
            self.or_sem.at[lands],
            {"z": other // NY, "y": lax.rem(other, NY)},
        )

    def each_in(self, j, do):
        def body(k, carry):
            other = j * self.span + lax.rem(self.ri + k, self.span)

            @pl.when(other != self.ri)
            def _():
                do(other)

            return carry

        lax.fori_loop(0, self.span, body, 0)

    def out_(self, st):
        self.s[2, self.ri, self.xi, :, self.lanes()] = self.fin[self.ri]
        self.each_other(lambda o: self.out_copy(o, True).wait_recv())

    def run(self):
        for c in self.w_copies:
            c.start()
        for event in ORDER:
            name, rest = event[0], event[1:]
            if name == "halo":
                self.halo_copy(*rest).start()
            elif name in ("in", "out"):
                getattr(self, name + "_")(*rest)
            else:
                getattr(self, name)(*rest)
        copy = pltpu.make_async_copy(self.s.at[2], self.out, self.l_sem.at[7])
        copy.start()
        for i in range(len(ITEMS)):
            for k in GATHER_KEYS:
                for d in "pm":
                    self.g_copy(i, k, d).wait_send()
        self.each_other(lambda o: self.in_copy(o).wait_send())
        self.each_other(lambda o: self.out_copy(o).wait_send())
        for j in range(CHUNKS):
            for which in range(3):
                for k in SHARE_KEYS:
                    self.share_copy(which, j, k).wait_send()
            for l in range(2):
                for k in SUM_KEYS:
                    self.sum_copy(l, j, k).wait_send()
        copy.wait()


def kernel(*refs):
    Program(refs).run()


def per_device(
    tokens, norm_gain, up_weight, gate_weight, up_scale, gate_scale, up_taps, gate_taps,
    down_weight, down_scale,
):
    bf16, f32 = jnp.bfloat16, jnp.float32
    w_in = jnp.stack(
        [w[l] for l in range(2) for w in (up_weight, gate_weight, down_weight)]
    ).astype(bf16)
    scale = lax.dynamic_index_in_dim(
        down_scale.reshape(2, NR, NX, 16), lax.axis_index("x"), axis=2, keepdims=False
    )
    scale = jnp.broadcast_to(scale[..., None], (2, NR, 16, 128))
    vmem, hbm = pl.BlockSpec(memory_space=pltpu.VMEM), pl.BlockSpec(memory_space=pl.ANY)
    dma = pltpu.SemaphoreType.DMA
    n = len(ITEMS)
    out = pl.pallas_call(
        kernel,
        out_shape=jax.ShapeDtypeStruct((NR, 4, 16, 512), bf16),
        in_specs=[hbm, hbm] + [vmem] * 6,
        out_specs=hbm,
        scratch_shapes=[
            pltpu.VMEM((6, NZ, NY, 64, 768), bf16),
            pltpu.VMEM((3, NR, 4, 16, 512), bf16),
            pltpu.VMEM((512, 2048), bf16),
            pltpu.VMEM((2, 520, 768), f32),
            pltpu.VMEM((2, 2, 8, 768), f32),
            pltpu.VMEM((512, 768), bf16),
            pltpu.VMEM((2, NR, 4, 16, 512), bf16),
            pltpu.VMEM((2, NR, 4, 16, 256), bf16),
            pltpu.VMEM((2, NR, 4, 16, 256), bf16),
            pltpu.VMEM((2, 2, NR // 2, 16, 256), bf16),
            pltpu.VMEM((2, 2, NR, 16, 256), bf16),
            pltpu.VMEM((NR, 16, 256), bf16),
            dma((8,)),
            dma((n, 24)), dma((n, 24)),
            dma((NR,)), dma((NR,)),
            dma((3, CHUNKS, 8)), dma((3, CHUNKS, 8)),
            dma((2, CHUNKS, 5)), dma((2, CHUNKS, 5)),
            dma((2, 3)), dma((2, 3)),
            dma((NR,)), dma((NR,)),
        ],
        compiler_params=pltpu.CompilerParams(
            has_side_effects=True, vmem_limit_bytes=60 * 2**20
        ),
    )(tokens, w_in, norm_gain, up_scale, gate_scale, up_taps, gate_taps, scale)
    return out.reshape(NR, 64, 512).transpose(1, 0, 2).reshape(64, NR * 512)


def solution(mesh):
    torus = Mesh(mesh.devices.reshape(NZ, NY, NX, 2), ("z", "y", "x", "c"))
    ra, cb = ("z", "y"), ("x", "c")
    placed = (
        P(ra, None),
        P(),
        P(None, ra, cb),
        P(None, ra, cb),
        P(None, cb),
        P(None, cb),
        P(None, None, cb),
        P(None, None, cb),
        P(None, ra, cb),
        P(),
    )
    return jax.shard_map(
        per_device, mesh=torus, in_specs=placed, out_specs=P(ra, None), check_vma=False
    )
```

```python
import jax
import jax.numpy as jnp
from jax import lax
from jax.experimental import pallas as pl
from jax.experimental.pallas import tpu as pltpu
from jax.sharding import Mesh
from jax.sharding import PartitionSpec as P

MESH = pl.DeviceIdType.MESH
EPS = 1e-06
RESIDUAL = 0.5
NZ, NY, NX = 8, 4, 4
NR = NZ * NY

ITEMS = [(0, 0, 384, 768), (1, 0, 256, 768), (2, 0, 256, 768), (3, 0, 384, 768), (4, 0, 256, 768), (5, 0, 256, 768)]
PAIR_KEYS = ("Ay1", "Ay2", "Az1", "Az2", "Az3", "Az4", "Bz1", "Bz2", "Bz3", "Bz4")
KEY = {k + d: i for i, (k, d) in enumerate([(k, d) for k in PAIR_KEYS for d in "pm"])}
for _k, _name in enumerate(("By1", "By2")):
    for _slot in range(NZ):
        for _d in range(2):
            KEY[_name + "pm"[_d], _slot] = 20 + 16 * _k + 2 * _slot + _d
SHARE_KEYS = {k: i for i, k in enumerate(("X1p", "X1m", "X2p", "X2m", "D0", "D1", "D2", "D3"))}
SUM_KEYS = {k: i for i, k in enumerate(("D", "Ap", "Am", "Bp", "Bm"))}

NEAR = ((0, 4), (4, 8), (12, 8), (20, 8), (28, 4))
HALVES = ((0, 16), (16, 16))
SHARE_CHUNKS = (HALVES, HALVES, NEAR)
SUM_CHUNKS = (HALVES, NEAR)


def offset(slot):
    return (slot + 1) // 2 * (2 * (slot % 2) - 1)


def slots_at(distance):
    return (0,) if distance == 0 else (7,) if distance == 4 else (2 * distance - 1, 2 * distance)


def opposite(slot):
    return slot if slot in (0, 7) else slot + 1 if slot % 2 else slot - 1


ORDER = [
    ("A", 2, 0), ("B", 1, 0), ("B", 3, 0), ("B", 5, 0), ("B", 2, 0), ("A", 0, 0), ("A", 1, 0),
    ("in", 0), ("A", 2, 1), ("A", 3, 0), ("A", 1, 1), ("B", 2, 1), ("B", 4, 0), ("A", 3, 1),
    ("B", 0, 0), ("A", 0, 1), ("A", 1, 2), ("A", 2, 2), ("B", 0, 1), ("B", 1, 1), ("in", 1),
    ("share", 0, 1, 0), ("A", 0, 2), ("B", 2, 2), ("B", 1, 2), ("B", 0, 2), ("A", 1, 3),
    ("C", 1, 1), ("A", 0, 3), ("A", 4, 0), ("B", 3, 1), ("B", 0, 3), ("C", 1, 0), ("A", 4, 1),
    ("C", 1, 2), ("C", 0, 1), ("B", 1, 3), ("share", 0, 0, 0), ("B", 4, 1), ("share", 0, 1, 1),
    ("A", 0, 4), ("B", 0, 4), ("A", 1, 4), ("A", 2, 3), ("share", 0, 1, 2), ("C", 0, 2),
    ("share", 0, 1, 3), ("C", 0, 3), ("B", 1, 4), ("C", 2, 1), ("B", 2, 3), ("E", 1, 2),
    ("share", 0, 0, 1), ("A", 0, 5), ("C", 2, 0), ("E", 0, 1), ("A", 2, 4), ("B", 3, 2),
    ("A", 1, 5), ("C", 2, 2), ("C", 0, 4), ("share", 0, 0, 2), ("E", 1, 1), ("C", 0, 0),
    ("C", 1, 4), ("share", 0, 0, 3), ("prep", 0), ("E", 1, 0), ("A", 3, 2), ("A", 2, 5),
    ("A", 0, 6), ("C", 1, 3), ("B", 2, 4), ("E", 2, 2), ("A", 5, 0), ("A", 4, 2), ("E", 1, 4),
    ("A", 1, 6), ("E", 0, 3), ("E", 0, 4), ("E", 2, 1), ("E", 2, 0), ("E", 0, 2), ("E", 0, 0),
    ("C", 3, 1), ("C", 2, 3), ("E", 1, 3), ("C", 3, 0), ("ug", 0, 0), ("ug", 0, 1), ("ug", 0, 2),
    ("halo", 0, 1), ("halo", 0, 0), ("halo", 0, 2), ("B", 5, 1), ("C", 2, 4), ("B", 3, 3),
    ("A", 3, 3), ("E", 2, 3), ("B", 4, 2), ("A", 5, 1), ("conv", 0), ("down", 0, 0), ("A", 2, 6),
    ("sum", 0, 0, 0), ("sum", 0, 0, 1), ("A", 4, 3), ("E", 2, 4), ("down", 0, 1), ("B", 5, 2),
    ("sum", 0, 1, 0), ("sum", 0, 1, 1), ("E", 3, 0), ("B", 3, 4), ("B", 4, 3), ("C", 5, 1),
    ("sum", 0, 0, 2), ("A", 5, 2), ("C", 3, 3), ("sum", 0, 1, 2), ("B", 4, 4), ("A", 3, 4),
    ("scale",), ("sum", 0, 0, 3), ("C", 4, 3), ("A", 4, 4), ("C", 4, 1), ("share", 1, 0, 0),
    ("sum", 0, 1, 3), ("share", 1, 1, 0), ("C", 3, 2), ("A", 3, 5), ("B", 5, 3), ("C", 4, 0),
    ("A", 5, 3), ("share", 1, 0, 1), ("share", 1, 1, 1), ("C", 3, 4), ("C", 4, 4), ("A", 4, 5),
    ("C", 4, 2), ("E", 4, 3), ("E", 3, 1), ("E", 5, 1), ("share", 1, 0, 2), ("C", 5, 2),
    ("E", 4, 1), ("E", 3, 2), ("B", 5, 4), ("E", 3, 3), ("A", 3, 6), ("share", 1, 1, 2),
    ("E", 3, 4), ("C", 5, 3), ("share", 1, 0, 3), ("A", 5, 4), ("E", 4, 4), ("share", 1, 1, 3),
    ("prep", 1), ("A", 4, 6), ("E", 4, 0), ("E", 4, 2), ("ug", 1, 0), ("halo", 1, 0), ("ug", 1, 1),
    ("halo", 1, 1), ("ug", 1, 2), ("halo", 1, 2), ("E", 5, 3), ("E", 5, 2), ("C", 5, 0),
    ("C", 5, 4), ("A", 5, 5), ("conv", 1), ("down", 1, 3), ("sum", 1, 3, 0), ("down", 1, 2),
    ("sum", 1, 2, 0), ("down", 1, 1), ("sum", 1, 1, 0), ("sum", 1, 3, 1), ("E", 5, 0),
    ("down", 1, 0), ("sum", 1, 0, 0), ("sum", 1, 2, 1), ("sum", 1, 1, 1), ("sum", 1, 0, 1),
    ("A", 5, 6), ("sum", 1, 3, 2), ("sum", 1, 2, 2), ("E", 5, 4), ("down", 1, 4), ("sum", 1, 4, 0),
    ("sum", 1, 4, 1), ("sum", 1, 0, 2), ("sum", 1, 1, 2), ("sum", 1, 3, 3), ("sum", 1, 2, 3),
    ("sum", 1, 4, 2), ("sum", 1, 0, 3), ("sum", 1, 1, 3), ("sum", 1, 4, 3), ("out", 3),
    ("share", 2, 3, 0), ("out", 2), ("share", 2, 2, 0), ("out", 1), ("share", 2, 1, 0), ("out", 0),
    ("share", 2, 0, 0), ("share", 2, 3, 1), ("out", 4), ("share", 2, 4, 0), ("share", 2, 2, 1),
    ("share", 2, 0, 1), ("share", 2, 1, 1), ("share", 2, 4, 1), ("share", 2, 3, 2),
    ("share", 2, 3, 3), ("share", 2, 0, 2), ("share", 2, 2, 2), ("share", 2, 1, 2),
    ("share", 2, 4, 2), ("share", 2, 1, 3), ("share", 2, 0, 3), ("fin", 0), ("fin", 3),
    ("share", 2, 2, 3), ("fin", 2), ("fin", 1), ("share", 2, 4, 3), ("fin", 4),
]


class Program:
    def __init__(self, refs):
        (
            self.tok, self.wu, self.wg, self.wd, self.gain, self.us, self.gs, self.ut, self.gt,
            self.ds, self.out, self.stage, self.scales,
            self.w, self.s, self.x, self.pre, self.halo, self.hid, self.part, self.rd, self.q,
            self.rh, self.rf, self.fin_,
            self.l_sem, self.gs_sem, self.gr_sem, self.is_sem, self.ir_sem, self.ss_sem, self.sr_sem,
            self.us_sem, self.ur_sem, self.hs_sem, self.hr_sem, self.os_sem, self.or_sem,
        ) = refs
        self.zi, self.yi = lax.axis_index("z"), lax.axis_index("y")
        self.xi, self.ci = lax.axis_index("x"), lax.axis_index("c")
        self.ri = self.zi * NY + self.yi
        self.w_copies = [
            pltpu.make_async_copy((self.wu, self.wg, self.wd)[m % 3].at[m // 3], self.stage.at[m], self.l_sem.at[m])
            for m in range(6)
        ]

    def z_of(self, slot):
        return lax.rem(self.zi + offset(slot) + NZ, NZ)

    def enter(self):
        for c in self.w_copies:
            c.start()
        barrier = pltpu.get_barrier_semaphore()

        def tell(to):
            pl.semaphore_signal(barrier, inc=1, device_id=to, device_id_type=MESH)

        tell(self.step_to("c", "p"))
        tell(self.step_to("x", "p"))
        tell(self.step_to("x", "m"))
        self.each_other(lambda o: tell({"z": o // NY, "y": lax.rem(o, NY)}))
        for m in range(6):
            self.w_copies[m].wait()
            self.w[m, self.zi, self.yi] = self.stage[m].astype(jnp.bfloat16)
        pl.semaphore_wait(barrier, NR + 2)

    def gather_region(self, i, key, d, slot, recv):
        m, c0, c1, c2 = ITEMS[i]
        sign = 1 if d == "p" else -1
        hop = int(key[2])
        back = hop if recv else hop - 1
        first, second = pl.ds(c0, c1 - c0), pl.ds(c1, c2 - c1)
        z = lax.rem(self.zi - sign * back + NZ, NZ)
        y = lax.rem(self.yi - sign * back + NY, NY)
        half = pl.ds(0 if d == "p" else 32, 32)
        w = self.w.at[m]
        if key[:2] == "Ay":
            return w.at[self.zi, y, half if hop == 2 else slice(None), first]
        if key[:2] == "Az":
            if hop == 4:
                return w.at[z, pl.ds(0 if d == "p" else 2, 2), :, first]
            return w.at[z, :, :, first]
        if key[:2] == "Bz":
            return w.at[z, self.yi, half if hop == 4 else slice(None), second]
        return w.at[self.z_of(slot), y, half if hop == 2 else slice(None), second]

    def step_to(self, link, d):
        if link == "z":
            return {"z": lax.rem(self.zi + (1 if d == "p" else NZ - 1), NZ)}
        if link == "y":
            return {"y": lax.rem(self.yi + (1 if d == "p" else NY - 1), NY)}
        if link == "x":
            return {"x": lax.rem(self.xi + (1 if d == "p" else NX - 1), NX)}
        return {"c": 1 - self.ci}

    @staticmethod
    def remote(src, dst, send, recv, to):
        return pltpu.make_async_remote_copy(
            src_ref=src, dst_ref=dst, send_sem=send, recv_sem=recv, device_id=to, device_id_type=MESH
        )

    def g_copy(self, i, key, d, slot=None, recv=False):
        region = self.gather_region(i, key, d, slot, recv)
        k = KEY[key + d] if slot is None else KEY[key + d, slot]
        return self.remote(
            region, region, self.gs_sem.at[i, k], self.gr_sem.at[i, k], self.step_to(key[1], d)
        )

    def g_send(self, i, key, slots=(None,)):
        for slot in slots:
            for d in "pm":
                self.g_copy(i, key, d, slot).start()

    def g_wait(self, i, key, slots=(None,)):
        for slot in slots:
            for d in "pm":
                self.g_copy(i, key, d, slot, True).wait_recv()

    def g_forward(self, i, came, goes, slots=(None,)):
        for slot in slots:
            for d in "pm":
                self.g_copy(i, came, d, slot, True).wait_recv()
                self.g_copy(i, goes, d, slot).start()

    def A(self, i, st):
        if st == 0:
            self.g_send(i, "Ay1")
        elif st == 1:
            self.g_forward(i, "Ay1", "Ay2")
        elif st == 2:
            self.g_wait(i, "Ay2")
            self.g_send(i, "Az1")
        elif st < 6:
            self.g_forward(i, f"Az{st - 2}", f"Az{st - 1}")
        else:
            self.g_wait(i, "Az4")

    def B(self, i, st):
        if st == 0:
            self.g_send(i, "Bz1")
        elif st < 4:
            self.g_forward(i, f"Bz{st}", f"Bz{st + 1}")
        else:
            self.g_wait(i, "Bz4")
        self.g_send(i, "By1", slots_at(st))

    def C(self, i, distance):
        self.g_forward(i, "By1", "By2", slots_at(distance))

    def E(self, i, distance):
        self.g_wait(i, "By2", slots_at(distance))

    def lanes(self, own=True):
        c = self.ci if own else 1 - self.ci
        return pl.ds(pl.multiple_of(c * 256, 256), 256)

    def in_own(self):
        cols = pl.ds(pl.multiple_of(self.ri * 512 + self.ci * 256, 256), 256)
        rows = pl.ds(pl.multiple_of(self.xi * 16, 16), 16)
        return pltpu.make_async_copy(
            self.tok.at[rows, cols], self.s.at[0, self.ri, self.xi, :, self.lanes()], self.l_sem.at[6]
        )

    def in_copy(self, other, recv=False):
        cols = pl.ds(pl.multiple_of(other * 512 + self.ci * 256, 256), 256)
        rows = pl.ds(pl.multiple_of(self.xi * 16, 16), 16)
        lands = other if recv else self.ri
        return self.remote(
            self.tok.at[rows, cols],
            self.s.at[0, lands, self.xi, :, self.lanes()],
            self.is_sem.at[other],
            self.ir_sem.at[lands],
            {"z": other // NY, "y": lax.rem(other, NY)},
        )

    def each_other(self, do):
        def body(k, carry):
            do(lax.rem(self.ri + k, NR))
            return carry

        lax.fori_loop(1, NR, body, 0)

    def in_(self, st):
        if st == 0:
            self.in_own().start()
            self.each_other(lambda o: self.in_copy(o).start())
        else:
            self.in_own().wait()
            self.each_other(lambda o: self.in_copy(o, True).wait_recv())

    def share_copy(self, which, j, key, recv=False):
        lo, n = SHARE_CHUNKS[which][j]
        if key[0] == "X":
            sign = 1 if key[2] == "p" else -1
            hop = int(key[1])
            back = hop if recv else hop - 1
            x = lax.rem(self.xi - sign * back + NX, NX)
            if hop == 2:
                n = n // 2
                lo += 0 if key[2] == "p" else n
            lanes, to = self.lanes(), self.step_to("x", key[2])
        else:
            off = {"D0": 0, "D1": NX - 1, "D2": 1, "D3": 2}[key]
            x = lax.rem(self.xi + off, NX)
            lanes, to = self.lanes(not recv), self.step_to("c", "p")
        region = self.s.at[which, pl.ds(lo, n), x, :, lanes]
        k = SHARE_KEYS[key]
        return self.remote(
            region, region, self.ss_sem.at[which, j, k], self.sr_sem.at[which, j, k], to
        )

    def share(self, which, j, st):
        def start(*keys):
            for k in keys:
                self.share_copy(which, j, k).start()

        def wait(*keys):
            for k in keys:
                self.share_copy(which, j, k, True).wait_recv()

        if st == 0:
            start("X1p", "X1m", "D0")
        elif st == 1:
            wait("X1p")
            start("X2p", "D1")
            wait("X1m")
            start("X2m", "D2")
        elif st == 2:
            wait("X2p", "X2m")
            start("D3")
        else:
            wait("D0", "D1", "D2", "D3")

    def prep(self, l):
        def body(k, acc):
            block = self.s[l, pl.ds(k * 4, 4)].reshape(256, 512)
            t = block.T.astype(jnp.float32)
            z = k if l == 0 else self.z_of(k)
            cols = pl.ds(pl.multiple_of(z * 256, 256), 256)
            self.x[:, cols] = (t * self.gain[l : l + 1, cols]).astype(jnp.bfloat16)
            sq = t * t
            return acc + sq[:, :128] + sq[:, 128:]

        acc = lax.fori_loop(0, 8, body, jnp.zeros((512, 128), jnp.float32))
        mean = jnp.sum(acc, axis=1, keepdims=True) * (1.0 / 2048)
        self.inverse = lax.rsqrt(mean + EPS)

    def ug(self, l, n):
        cols = slice(n * 256, n * 256 + 256)
        for k, scale in ((0, self.us), (1, self.gs)):
            w = self.w[3 * l + k, :, :, :, cols].reshape(2048, 256)
            raw = jnp.dot(self.x[...], w, preferred_element_type=jnp.float32)
            self.pre[k, 8:520, cols] = raw * self.inverse * scale[l : l + 1, cols]

    def halo_copy(self, l, n):
        cols = pl.ds(n * 256, 256)
        wrap = jnp.where(self.yi == NY - 1, 1, 0)
        to = {"z": lax.rem(self.zi + wrap, NZ), "y": lax.rem(self.yi + 1, NY)}
        return self.remote(
            self.pre.at[:, pl.ds(512, 8), cols], self.halo.at[l, :, :, cols],
            self.hs_sem.at[l, n], self.hr_sem.at[l, n], to,
        )

    def conv(self, l):
        for n in range(3):
            self.halo_copy(l, n).wait_recv()
        first = self.ri == 0
        for n in range(6):
            cols = slice(n * 128, n * 128 + 128)
            both = []
            for k, taps in ((0, self.ut), (1, self.gt)):
                before = self.halo[l, k, :, cols]
                self.pre[k, 0:8, cols] = jnp.where(first, jnp.zeros_like(before), before)
                total = taps[0, l : l + 1, cols] * self.pre[k, 6:518, cols]
                total += taps[1, l : l + 1, cols] * self.pre[k, 7:519, cols]
                total += taps[2, l : l + 1, cols] * self.pre[k, 8:520, cols]
                both.append(total)
            up, gate = both
            self.hid[:, cols] = (gate / (1.0 + jnp.exp(-gate)) * up).astype(jnp.bfloat16)
        for n in range(3):
            self.halo_copy(l, n).wait_send()

    def scale(self):
        def body(k, carry):
            cols = pl.ds(pl.multiple_of(k * 128, 128), 128)
            for l in range(2):
                row = jnp.broadcast_to(self.ds[l : l + 1, cols], (128, 128))
                self.scales[l, pl.ds(k * 2, 2)] = row.T.reshape(2, 4, 16, 128)
            return carry

        lax.fori_loop(0, 16, body, 0)

    def down(self, l, j):
        def body(slot, carry):
            w = self.w[3 * l + 2, self.z_of(slot)].reshape(256, 768)
            part = lax.dot_general(
                w, self.hid[...], (((1,), (1,)), ((), ())), preferred_element_type=jnp.float32
            )
            self.part[l, pl.ds(slot * NY, NY)] = part.astype(jnp.bfloat16).reshape(NY, 4, 16, 512)
            return carry

        lo, n = SUM_CHUNKS[l][j]
        lax.fori_loop(lo // NY, (lo + n) // NY, body, 0)

    def sum_copy(self, l, j, key):
        lo, n = SUM_CHUNKS[l][j]
        h = n // 2
        k = SUM_KEYS[key]
        sems = (self.us_sem.at[l, j, k], self.ur_sem.at[l, j, k])
        if key == "D":
            return self.remote(
                self.part.at[l, pl.ds(lo, n), :, :, self.lanes(False)],
                self.rd.at[l, pl.ds(lo, n)], *sems, self.step_to("c", "p"),
            )
        d = key[1]
        if key[0] == "A":
            first = lo + (0 if d == "p" else h)
            return self.remote(
                self.q.at[l, pl.ds(first, h), lax.rem(self.xi + 2, NX)],
                self.rh.at[l, 0 if d == "p" else 1, pl.ds(lo // 2, h)], *sems, self.step_to("x", d),
            )
        return self.remote(
            self.q.at[l, pl.ds(lo, n), lax.rem(self.xi + (1 if d == "p" else NX - 1), NX)],
            self.rf.at[l, 0 if d == "p" else 1, pl.ds(lo, n)], *sems, self.step_to("x", d),
        )

    def sum(self, l, j, st):
        lo, n = SUM_CHUNKS[l][j]
        h = n // 2
        f32, bf16 = jnp.float32, jnp.bfloat16
        rows = pl.ds(lo, n)
        if st == 0:
            self.sum_copy(l, j, "D").start()
        elif st == 1:
            self.sum_copy(l, j, "D").wait_recv()
            mine = self.part[l, rows, :, :, self.lanes()].astype(f32)
            self.q[l, rows] = (mine + self.rd[l, rows].astype(f32)).astype(bf16)
            self.sum_copy(l, j, "Ap").start()
            self.sum_copy(l, j, "Am").start()
        elif st == 2:
            for d, key in ((1, "p"), (-1, "m")):
                self.sum_copy(l, j, "A" + key).wait_recv()
                x = lax.rem(self.xi + d + NX, NX)
                part = pl.ds(lo + (0 if key == "p" else h), h)
                came = self.rh[l, 0 if key == "p" else 1, pl.ds(lo // 2, h)].astype(f32)
                self.q[l, part, x] = (self.q[l, part, x].astype(f32) + came).astype(bf16)
                self.sum_copy(l, j, "B" + key).start()
        else:
            self.sum_copy(l, j, "Bp").wait_recv()
            self.sum_copy(l, j, "Bm").wait_recv()
            for slot in range(lo // NY, (lo + n) // NY):
                near, place = pl.ds(slot * NY, NY), pl.ds(self.z_of(slot) * NY, NY)
                total = self.q[l, near, self.xi].astype(f32)
                total += self.rf[l, 0, near].astype(f32) + self.rf[l, 1, near].astype(f32)
                scale = self.scales[l, place, self.xi]
                scale = jnp.concatenate([scale, scale], axis=2)
                old = self.s[l, place if l == 0 else near, self.xi, :, self.lanes()].astype(f32)
                new = (total * scale + RESIDUAL * old).astype(bf16)
                if l == 0:
                    self.s[1, near, self.xi, :, self.lanes()] = new
                else:
                    self.fin_[near] = new
            if l == 1:
                self.each_out(j, lambda slot, y: self.out_copy(slot, y).start())

    def out_copy(self, slot, y, recv=False):
        if recv:
            here, there = slot * NY + y, slot * NY + y
        else:
            here, there = slot * NY + y, opposite(slot) * NY + self.yi
        return self.remote(
            self.fin_.at[here],
            self.s.at[2, there, self.xi, :, self.lanes()],
            self.os_sem.at[here],
            self.or_sem.at[there],
            {"z": self.z_of(slot), "y": y},
        )

    def each_out(self, j, do):
        lo, n = SUM_CHUNKS[1][j]
        for slot in range(lo // NY, (lo + n) // NY):
            for k in range(1 if slot == 0 else 0, NY):
                do(slot, lax.rem(self.yi + k, NY))

    def out_(self, j):
        if j == 0:
            self.s[2, self.yi, self.xi, :, self.lanes()] = self.fin_[self.yi]
        self.each_out(j, lambda slot, y: self.out_copy(slot, y, True).wait_recv())

    def fin_copy(self, slot):
        return pltpu.make_async_copy(
            self.s.at[2, pl.ds(slot * NY, NY)],
            self.out.at[pl.ds(self.z_of(slot) * NY, NY)],
            self.l_sem.at[7 + slot],
        )

    def fin(self, j):
        lo, n = SHARE_CHUNKS[2][j]
        for slot in range(lo // NY, (lo + n) // NY):
            self.fin_copy(slot).start()

    def run(self):
        self.enter()
        for event in ORDER:
            name, rest = event[0], event[1:]
            if name == "halo":
                self.halo_copy(*rest).start()
            elif name in ("in", "out"):
                getattr(self, name + "_")(*rest)
            else:
                getattr(self, name)(*rest)
        for i in range(len(ITEMS)):
            for k in PAIR_KEYS:
                for d in "pm":
                    self.g_copy(i, k, d).wait_send()
            for k in ("By1", "By2"):
                for slot in range(NZ):
                    for d in "pm":
                        self.g_copy(i, k, d, slot).wait_send()
        self.each_other(lambda o: self.in_copy(o).wait_send())
        for which in range(3):
            for j in range(len(SHARE_CHUNKS[which])):
                for k in SHARE_KEYS:
                    self.share_copy(which, j, k).wait_send()
        for l in range(2):
            for j in range(len(SUM_CHUNKS[l])):
                for k in SUM_KEYS:
                    self.sum_copy(l, j, k).wait_send()
        for j in range(len(SUM_CHUNKS[1])):
            self.each_out(j, lambda slot, y: self.out_copy(slot, y).wait_send())
        for slot in range(NZ):
            self.fin_copy(slot).wait()


def kernel(*refs):
    Program(refs).run()


def per_device(
    tokens, norm_gain, up_weight, gate_weight, up_scale, gate_scale, up_taps, gate_taps,
    down_weight, down_scale,
):
    bf16, f32 = jnp.bfloat16, jnp.float32
    vmem, hbm = pl.BlockSpec(memory_space=pltpu.VMEM), pl.BlockSpec(memory_space=pl.ANY)
    dma = pltpu.SemaphoreType.DMA
    n = len(ITEMS)
    out = pl.pallas_call(
        kernel,
        out_shape=jax.ShapeDtypeStruct((NR, 4, 16, 512), bf16),
        in_specs=[hbm] * 4 + [vmem] * 6,
        out_specs=hbm,
        scratch_shapes=[
            pltpu.VMEM((6, 64, 768), f32),
            pltpu.VMEM((2, NR, 4, 16, 128), f32),
            pltpu.VMEM((6, NZ, NY, 64, 768), bf16),
            pltpu.VMEM((3, NR, 4, 16, 512), bf16),
            pltpu.VMEM((512, 2048), bf16),
            pltpu.VMEM((2, 520, 768), f32),
            pltpu.VMEM((2, 2, 8, 768), f32),
            pltpu.VMEM((512, 768), bf16),
            pltpu.VMEM((2, NR, 4, 16, 512), bf16),
            pltpu.VMEM((2, NR, 4, 16, 256), bf16),
            pltpu.VMEM((2, NR, 4, 16, 256), bf16),
            pltpu.VMEM((2, 2, NR // 2, 16, 256), bf16),
            pltpu.VMEM((2, 2, NR, 16, 256), bf16),
            pltpu.VMEM((NR, 16, 256), bf16),
            dma((15,)),
            dma((n, 52)), dma((n, 52)),
            dma((NR,)), dma((NR,)),
            dma((3, 5, 8)), dma((3, 5, 8)),
            dma((2, 5, 5)), dma((2, 5, 5)),
            dma((2, 3)), dma((2, 3)),
            dma((NR,)), dma((NR,)),
        ],
        compiler_params=pltpu.CompilerParams(
            collective_id=0, has_side_effects=True, vmem_limit_bytes=60 * 2**20
        ),
    )(
        tokens, up_weight, gate_weight, down_weight, norm_gain, up_scale, gate_scale,
        up_taps.transpose(1, 0, 2), gate_taps.transpose(1, 0, 2), down_scale,
    )
    return out.reshape(NR, 64, 512).transpose(1, 0, 2).reshape(64, NR * 512)


def solution(mesh):
    torus = Mesh(mesh.devices.reshape(NZ, NY, NX, 2), ("z", "y", "x", "c"))
    ra, cb = ("z", "y"), ("x", "c")
    placed = (
        P(ra, None),
        P(),
        P(None, ra, cb),
        P(None, ra, cb),
        P(None, cb),
        P(None, cb),
        P(None, None, cb),
        P(None, None, cb),
        P(None, ra, cb),
        P(),
    )
    return jax.shard_map(
        per_device, mesh=torus, in_specs=placed, out_specs=P(ra, None), check_vma=False
    )
```

```python
import jax
import jax.numpy as jnp
from jax import lax
from jax.experimental import pallas as pl
from jax.experimental.pallas import tpu as pltpu
from jax.sharding import Mesh
from jax.sharding import PartitionSpec as P

MESH = pl.DeviceIdType.MESH
EPS = 1e-06
RESIDUAL = 0.5
NZ, NY, NX = 8, 4, 4
NR = NZ * NY

ITEMS = [(0, 0, 384, 768), (1, 0, 256, 768), (2, 0, 256, 768), (3, 0, 384, 768), (4, 0, 256, 768), (5, 0, 256, 768)]
PAIR_KEYS = ("Ay1", "Ay2", "Az1", "Az2", "Az3", "Az4", "Bz1", "Bz2", "Bz3", "Bz4")
KEY = {k: i for i, k in enumerate(PAIR_KEYS)}
for _k, _name in enumerate(("By1", "By2")):
    for _distance in range(5):
        KEY[_name, _distance] = 10 + 5 * _k + _distance

NEAR = ((0, 4), (4, 8), (12, 8), (20, 8), (28, 4))
HALVES = ((0, 16), (16, 16))
SHARE_CHUNKS = (HALVES, HALVES, NEAR)
SUM_CHUNKS = (HALVES, NEAR)
SHARE_SEMS = 3 * 9
SUM_SEMS = 3 * 7


def offset(slot):
    return (slot + 1) // 2 * (2 * (slot % 2) - 1)


def slots_at(distance):
    return (0,) if distance == 0 else (7,) if distance == 4 else (2 * distance - 1, 2 * distance)


def distance_of(slot):
    return (slot + 1) // 2


def opposite(slot):
    return slot if slot in (0, 7) else slot + 1 if slot % 2 else slot - 1


ORDER = [
    ("know", 0), ("A", 2, 0), ("know", 1), ("B", 1, 0), ("know", 2), ("B", 3, 0), ("know", 3),
    ("B", 5, 0), ("know", 4), ("B", 2, 0), ("know", 5), ("A", 0, 0), ("A", 1, 0), ("in", 0),
    ("A", 2, 1), ("A", 3, 0), ("A", 1, 1), ("B", 2, 1), ("B", 4, 0), ("A", 3, 1), ("B", 0, 0),
    ("A", 0, 1), ("A", 1, 2), ("A", 2, 2), ("B", 0, 1), ("B", 1, 1), ("in", 1), ("share", 0, 1, 0),
    ("A", 0, 2), ("B", 2, 2), ("B", 1, 2), ("B", 0, 2), ("A", 1, 3), ("C", 1, 1), ("A", 0, 3),
    ("A", 4, 0), ("B", 3, 1), ("B", 0, 3), ("C", 1, 0), ("A", 4, 1), ("C", 1, 2), ("C", 0, 1),
    ("B", 1, 3), ("share", 0, 0, 0), ("B", 4, 1), ("share", 0, 1, 1), ("A", 0, 4), ("B", 0, 4),
    ("A", 1, 4), ("A", 2, 3), ("share", 0, 1, 2), ("C", 0, 2), ("share", 0, 1, 3), ("C", 0, 3),
    ("B", 1, 4), ("C", 2, 1), ("B", 2, 3), ("E", 1, 2), ("share", 0, 0, 1), ("A", 0, 5),
    ("C", 2, 0), ("E", 0, 1), ("A", 2, 4), ("B", 3, 2), ("A", 1, 5), ("C", 2, 2), ("C", 0, 4),
    ("share", 0, 0, 2), ("E", 1, 1), ("C", 0, 0), ("C", 1, 4), ("share", 0, 0, 3), ("prep", 0),
    ("E", 1, 0), ("A", 3, 2), ("A", 2, 5), ("A", 0, 6), ("C", 1, 3), ("B", 2, 4), ("E", 2, 2),
    ("A", 5, 0), ("A", 4, 2), ("E", 1, 4), ("A", 1, 6), ("E", 0, 3), ("E", 0, 4), ("E", 2, 1),
    ("E", 2, 0), ("E", 0, 2), ("E", 0, 0), ("C", 3, 1), ("C", 2, 3), ("E", 1, 3), ("C", 3, 0),
    ("ug", 0, 0), ("ug", 0, 1), ("ug", 0, 2), ("halo", 0, 1), ("halo", 0, 0), ("halo", 0, 2),
    ("B", 5, 1), ("C", 2, 4), ("B", 3, 3), ("A", 3, 3), ("E", 2, 3), ("B", 4, 2), ("A", 5, 1),
    ("conv", 0), ("down", 0, 0), ("A", 2, 6), ("sum", 0, 0, 0), ("sum", 0, 0, 1), ("A", 4, 3),
    ("E", 2, 4), ("down", 0, 1), ("B", 5, 2), ("sum", 0, 1, 0), ("sum", 0, 1, 1), ("E", 3, 0),
    ("B", 3, 4), ("B", 4, 3), ("C", 5, 1), ("sum", 0, 0, 2), ("A", 5, 2), ("C", 3, 3),
    ("sum", 0, 1, 2), ("B", 4, 4), ("A", 3, 4), ("scale",), ("sum", 0, 0, 3), ("C", 4, 3),
    ("A", 4, 4), ("C", 4, 1), ("share", 1, 0, 0), ("sum", 0, 1, 3), ("share", 1, 1, 0), ("C", 3, 2),
    ("A", 3, 5), ("B", 5, 3), ("C", 4, 0), ("A", 5, 3), ("share", 1, 0, 1), ("share", 1, 1, 1),
    ("C", 3, 4), ("C", 4, 4), ("A", 4, 5), ("C", 4, 2), ("E", 4, 3), ("E", 3, 1), ("E", 5, 1),
    ("share", 1, 0, 2), ("C", 5, 2), ("E", 4, 1), ("E", 3, 2), ("B", 5, 4), ("E", 3, 3),
    ("A", 3, 6), ("share", 1, 1, 2), ("E", 3, 4), ("C", 5, 3), ("share", 1, 0, 3), ("A", 5, 4),
    ("E", 4, 4), ("share", 1, 1, 3), ("prep", 1), ("A", 4, 6), ("E", 4, 0), ("E", 4, 2),
    ("ug", 1, 0), ("halo", 1, 0), ("ug", 1, 1), ("halo", 1, 1), ("ug", 1, 2), ("halo", 1, 2),
    ("E", 5, 3), ("E", 5, 2), ("C", 5, 0), ("C", 5, 4), ("A", 5, 5), ("conv", 1), ("down", 1, 3),
    ("sum", 1, 3, 0), ("down", 1, 2), ("sum", 1, 2, 0), ("down", 1, 1), ("sum", 1, 1, 0),
    ("sum", 1, 3, 1), ("E", 5, 0), ("down", 1, 0), ("sum", 1, 0, 0), ("sum", 1, 2, 1),
    ("sum", 1, 1, 1), ("sum", 1, 0, 1), ("A", 5, 6), ("sum", 1, 3, 2), ("sum", 1, 2, 2),
    ("E", 5, 4), ("down", 1, 4), ("sum", 1, 4, 0), ("sum", 1, 4, 1), ("sum", 1, 0, 2),
    ("sum", 1, 1, 2), ("sum", 1, 3, 3), ("sum", 1, 2, 3), ("sum", 1, 4, 2), ("sum", 1, 0, 3),
    ("sum", 1, 1, 3), ("sum", 1, 4, 3), ("out", 3), ("share", 2, 3, 0), ("out", 2),
    ("share", 2, 2, 0), ("out", 1), ("share", 2, 1, 0), ("out", 0), ("share", 2, 0, 0),
    ("share", 2, 3, 1), ("out", 4), ("share", 2, 4, 0), ("share", 2, 2, 1), ("share", 2, 0, 1),
    ("share", 2, 1, 1), ("share", 2, 4, 1), ("share", 2, 3, 2), ("share", 2, 3, 3),
    ("share", 2, 0, 2), ("share", 2, 2, 2), ("share", 2, 1, 2), ("share", 2, 4, 2),
    ("share", 2, 1, 3), ("share", 2, 0, 3), ("fin", 0), ("fin", 3), ("share", 2, 2, 3), ("fin", 2),
    ("fin", 1), ("share", 2, 4, 3), ("fin", 4),
]


class Program:
    def __init__(self, refs):
        (
            self.tok, self.wu, self.wg, self.wd, self.gain, self.us, self.gs, self.ut, self.gt,
            self.ds, self.out, self.stage, self.scales,
            self.w, self.s, self.x, self.pre, self.halo, self.hid, self.part, self.rd, self.q,
            self.rh, self.rf, self.fin_,
            self.l_sem, self.g_send_sem, self.g_sem, self.i_send_sem, self.i_sem,
            self.s_send_sem, self.s_sem, self.u_send_sem, self.u_sem, self.h_send_sem, self.h_sem,
            self.o_send_sem, self.o_sem, self.know_sem,
        ) = refs
        self.zi, self.yi = lax.axis_index("z"), lax.axis_index("y")
        self.xi, self.ci = lax.axis_index("x"), lax.axis_index("c")
        self.ri = self.zi * NY + self.yi
        self.w_copies = [
            pltpu.make_async_copy((self.wu, self.wg, self.wd)[m % 3].at[m // 3], self.stage.at[m], self.l_sem.at[0])
            for m in range(6)
        ]

    def z_of(self, slot):
        return lax.rem(self.zi + offset(slot) + NZ, NZ)

    def enter(self):
        for c in self.w_copies:
            c.start()
        barrier = pltpu.get_barrier_semaphore()

        def tell(to):
            pl.semaphore_signal(barrier, inc=1, device_id=to, device_id_type=MESH)

        tell(self.step_to("c", "p"))
        for link in "xyz":
            for d in "pm":
                tell(self.step_to(link, d))
        pltpu.make_async_copy(self.stage, self.stage, self.l_sem.at[0]).wait()
        for m in range(6):
            self.w[m, self.ri] = self.stage[m].astype(jnp.bfloat16)
        pl.semaphore_wait(barrier, 7)

    def know(self, k):
        if k > 0:
            pl.semaphore_wait(self.know_sem.at[k - 1], 2)
        if k < 5:
            for d in "pm":
                pl.semaphore_signal(
                    self.know_sem.at[k], inc=1, device_id=self.step_to("y" if k == 0 else "z", d),
                    device_id_type=MESH,
                )

    def gather_region(self, i, key, d, slot):
        m, c0, c1, c2 = ITEMS[i]
        sign = 1 if d == "p" else -1
        hop = int(key[2])
        back = hop - 1
        first, second = pl.ds(c0, c1 - c0), pl.ds(c1, c2 - c1)
        z = lax.rem(self.zi - sign * back + NZ, NZ)
        y = lax.rem(self.yi - sign * back + NY, NY)
        half = pl.ds(0 if d == "p" else 32, 32)
        w = self.w.at[m]
        if key[:2] == "Ay":
            return w.at[self.zi * NY + y, half if hop == 2 else slice(None), first]
        if key[:2] == "Az":
            if hop == 4:
                return w.at[pl.ds(z * NY + (0 if d == "p" else 2), 2), :, first]
            return w.at[pl.ds(z * NY, NY), :, first]
        if key[:2] == "Bz":
            return w.at[z * NY + self.yi, half if hop == 4 else slice(None), second]
        return w.at[self.z_of(slot) * NY + y, half if hop == 2 else slice(None), second]

    def step_to(self, link, d):
        if link == "z":
            return {"z": lax.rem(self.zi + (1 if d == "p" else NZ - 1), NZ)}
        if link == "y":
            return {"y": lax.rem(self.yi + (1 if d == "p" else NY - 1), NY)}
        if link == "x":
            return {"x": lax.rem(self.xi + (1 if d == "p" else NX - 1), NX)}
        return {"c": 1 - self.ci}

    @staticmethod
    def remote(src, dst, send, recv, to):
        return pltpu.make_async_remote_copy(
            src_ref=src, dst_ref=dst, send_sem=send, recv_sem=recv, device_id=to, device_id_type=MESH
        )

    def g_copy(self, i, key, d, slot=None):
        region = self.gather_region(i, key, d, slot)
        k = KEY[key] if slot is None else KEY[key, distance_of(slot)]
        return self.remote(
            region, region, self.g_send_sem.at[0], self.g_sem.at[i, k], self.step_to(key[1], d)
        )

    def g_send(self, i, key, slots=(None,)):
        for slot in slots:
            for d in "pm":
                self.g_copy(i, key, d, slot).start()

    def await_bytes(self, like, sem):
        pltpu.make_async_copy(like, like, sem).wait()

    def g_wait(self, i, key, distance=None):
        m, c0, c1, c2 = ITEMS[i]
        cols = pl.ds(c0, c1 - c0) if key[0] == "A" else pl.ds(c1, c2 - c1)
        shards = {"Ay1": 2, "Ay2": 1, "Az4": 4, "Bz4": 1}.get(key, 8 if key[:2] == "Az" else 2)
        k = KEY[key] if distance is None else KEY[key, distance]
        if distance is not None:
            shards = len(slots_at(distance)) * (2 if key == "By1" else 1)
        self.await_bytes(self.w.at[m, pl.ds(0, shards), :, cols], self.g_sem.at[i, k])

    def g_forward(self, i, came, goes):
        self.g_wait(i, came)
        self.g_send(i, goes)

    def A(self, i, st):
        if st == 0:
            self.g_send(i, "Ay1")
        elif st == 1:
            self.g_forward(i, "Ay1", "Ay2")
        elif st == 2:
            self.g_wait(i, "Ay2")
            self.g_send(i, "Az1")
        elif st < 6:
            self.g_forward(i, f"Az{st - 2}", f"Az{st - 1}")
        else:
            self.g_wait(i, "Az4")

    def B(self, i, st):
        if st == 0:
            self.g_send(i, "Bz1")
        elif st < 4:
            self.g_forward(i, f"Bz{st}", f"Bz{st + 1}")
        else:
            self.g_wait(i, "Bz4")
        self.g_send(i, "By1", slots_at(st))

    def C(self, i, distance):
        self.g_wait(i, "By1", distance)
        self.g_send(i, "By2", slots_at(distance))

    def E(self, i, distance):
        self.g_wait(i, "By2", distance)

    def lanes(self, own=True):
        c = self.ci if own else 1 - self.ci
        return pl.ds(pl.multiple_of(c * 256, 256), 256)

    def rows(self, x):
        return pl.ds(pl.multiple_of(x * 16, 16), 16)

    def in_own(self):
        cols = pl.ds(pl.multiple_of(self.ri * 512 + self.ci * 256, 256), 256)
        rows = pl.ds(pl.multiple_of(self.xi * 16, 16), 16)
        return pltpu.make_async_copy(
            self.tok.at[rows, cols], self.s.at[0, self.ri, self.rows(self.xi), self.lanes()], self.l_sem.at[1]
        )

    def in_copy(self, other):
        cols = pl.ds(pl.multiple_of(other * 512 + self.ci * 256, 256), 256)
        rows = pl.ds(pl.multiple_of(self.xi * 16, 16), 16)
        return self.remote(
            self.tok.at[rows, cols],
            self.s.at[0, self.ri, self.rows(self.xi), self.lanes()],
            self.i_send_sem.at[0],
            self.i_sem.at[0],
            {"z": other // NY, "y": lax.rem(other, NY)},
        )

    def each_other(self, do):
        def body(k, carry):
            do(lax.rem(self.ri + k, NR))
            return carry

        lax.fori_loop(1, NR, body, 0)

    def in_(self, st):
        if st == 0:
            self.in_own().start()
            self.each_other(lambda o: self.in_copy(o).start())
        else:
            self.in_own().wait()
            self.await_bytes(self.fin_.at[pl.ds(0, NR - 1)], self.i_sem.at[0])

    def share_copy(self, which, j, key):
        lo, n = SHARE_CHUNKS[which][j]
        sem = self.s_sem.at[(2 * which + j) * 3 + {"X1": 0, "X2": 1}.get(key[:2], 2)]
        if key[0] == "X":
            sign = 1 if key[2] == "p" else -1
            hop = int(key[1])
            x = lax.rem(self.xi - sign * (hop - 1) + NX, NX)
            if hop == 2:
                n = n // 2
                lo += 0 if key[2] == "p" else n
            to = self.step_to("x", key[2])
        else:
            x = lax.rem(self.xi + {"D0": 0, "D1": NX - 1, "D2": 1, "D3": 2}[key], NX)
            to = self.step_to("c", "p")
        region = self.s.at[which, pl.ds(lo, n), self.rows(x), self.lanes()]
        return self.remote(region, region, self.s_send_sem.at[0], sem, to)

    def share(self, which, j, st):
        lo, n = SHARE_CHUNKS[which][j]
        sem = (2 * which + j) * 3

        def start(*keys):
            for k in keys:
                self.share_copy(which, j, k).start()

        def arrived(quarters, k):
            like = self.s.at[which, pl.ds(lo, n), pl.ds(0, 16 * quarters), self.lanes()]
            self.await_bytes(like, self.s_sem.at[sem + k])

        if st == 0:
            start("X1p", "X1m", "D0")
        elif st == 1:
            arrived(2, 0)
            start("X2p", "X2m", "D1", "D2")
        elif st == 2:
            arrived(1, 1)
            start("D3")
        else:
            arrived(4, 2)

    def prep(self, l):
        def body(k, acc):
            block = self.s[l, pl.ds(k * 4, 4)].reshape(256, 512)
            t = block.T.astype(jnp.float32)
            z = k if l == 0 else self.z_of(k)
            cols = pl.ds(pl.multiple_of(z * 256, 256), 256)
            self.x[:, cols] = (t * self.gain[l : l + 1, cols]).astype(jnp.bfloat16)
            sq = t * t
            return acc + sq[:, :128] + sq[:, 128:]

        acc = lax.fori_loop(0, 8, body, jnp.zeros((512, 128), jnp.float32))
        mean = jnp.sum(acc, axis=1, keepdims=True) * (1.0 / 2048)
        self.inverse = lax.rsqrt(mean + EPS)

    def ug(self, l, n):
        cols = slice(n * 256, n * 256 + 256)
        for k, scale in ((0, self.us), (1, self.gs)):
            w = self.w[3 * l + k, :, :, cols].reshape(2048, 256)
            raw = jnp.dot(self.x[...], w, preferred_element_type=jnp.float32)
            self.pre[k, 8:520, cols] = raw * self.inverse * scale[l : l + 1, cols]

    def halo_copy(self, l, n):
        cols = pl.ds(n * 256, 256)
        wrap = jnp.where(self.yi == NY - 1, 1, 0)
        to = {"z": lax.rem(self.zi + wrap, NZ), "y": lax.rem(self.yi + 1, NY)}
        return self.remote(
            self.pre.at[:, pl.ds(512, 8), cols], self.halo.at[l, :, :, cols],
            self.h_send_sem.at[l], self.h_sem.at[l], to,
        )

    def conv(self, l):
        self.await_bytes(self.halo.at[l], self.h_sem.at[l])
        first = self.ri == 0
        for n in range(6):
            cols = slice(n * 128, n * 128 + 128)
            both = []
            for k, taps in ((0, self.ut), (1, self.gt)):
                before = self.halo[l, k, :, cols]
                self.pre[k, 0:8, cols] = jnp.where(first, jnp.zeros_like(before), before)
                total = taps[0, l : l + 1, cols] * self.pre[k, 6:518, cols]
                total += taps[1, l : l + 1, cols] * self.pre[k, 7:519, cols]
                total += taps[2, l : l + 1, cols] * self.pre[k, 8:520, cols]
                both.append(total)
            up, gate = both
            self.hid[:, cols] = (gate / (1.0 + jnp.exp(-gate)) * up).astype(jnp.bfloat16)
        self.await_bytes(self.halo.at[l], self.h_send_sem.at[l])

    def scale(self):
        def body(k, carry):
            cols = pl.ds(pl.multiple_of(k * 128, 128), 128)
            for l in range(2):
                row = jnp.broadcast_to(self.ds[l : l + 1, cols], (128, 128))
                self.scales[l, pl.ds(k * 2, 2)] = row.T.reshape(2, 4, 16, 128)
            return carry

        lax.fori_loop(0, 16, body, 0)

    def down(self, l, j):
        def body(slot, carry):
            w = self.w[3 * l + 2, pl.ds(self.z_of(slot) * NY, NY)].reshape(256, 768)
            part = lax.dot_general(
                w, self.hid[...], (((1,), (1,)), ((), ())), preferred_element_type=jnp.float32
            )
            self.part[l, pl.ds(slot * NY, NY)] = part.astype(jnp.bfloat16).reshape(NY, 4, 16, 512)
            return carry

        lo, n = SUM_CHUNKS[l][j]
        lax.fori_loop(lo // NY, (lo + n) // NY, body, 0)

    def sum_copy(self, l, j, key):
        lo, n = SUM_CHUNKS[l][j]
        h = n // 2
        k = (2 * l + j) * 3 + "DAB".index(key[0])
        sems = (self.u_send_sem.at[0], self.u_sem.at[k])
        if key == "D":
            return self.remote(
                self.part.at[l, pl.ds(lo, n), :, :, self.lanes(False)],
                self.rd.at[l, pl.ds(lo, n)], *sems, self.step_to("c", "p"),
            )
        d = key[1]
        if key[0] == "A":
            first = lo + (0 if d == "p" else h)
            return self.remote(
                self.q.at[l, pl.ds(first, h), lax.rem(self.xi + 2, NX)],
                self.rh.at[l, 0 if d == "p" else 1, pl.ds(lo // 2, h)], *sems, self.step_to("x", d),
            )
        return self.remote(
            self.q.at[l, pl.ds(lo, n), lax.rem(self.xi + (1 if d == "p" else NX - 1), NX)],
            self.rf.at[l, 0 if d == "p" else 1, pl.ds(lo, n)], *sems, self.step_to("x", d),
        )

    def sum(self, l, j, st):
        lo, n = SUM_CHUNKS[l][j]
        h = n // 2
        f32, bf16 = jnp.float32, jnp.bfloat16
        rows = pl.ds(lo, n)
        sem = (2 * l + j) * 3
        if st == 0:
            self.sum_copy(l, j, "D").start()
        elif st == 1:
            self.await_bytes(self.rd.at[l, rows], self.u_sem.at[sem])
            mine = self.part[l, rows, :, :, self.lanes()].astype(f32)
            self.q[l, rows] = (mine + self.rd[l, rows].astype(f32)).astype(bf16)
            self.sum_copy(l, j, "Ap").start()
            self.sum_copy(l, j, "Am").start()
        elif st == 2:
            self.await_bytes(self.rh.at[l, :, pl.ds(lo // 2, h)], self.u_sem.at[sem + 1])
            for d, key in ((1, "p"), (-1, "m")):
                x = lax.rem(self.xi + d + NX, NX)
                part = pl.ds(lo + (0 if key == "p" else h), h)
                came = self.rh[l, 0 if key == "p" else 1, pl.ds(lo // 2, h)].astype(f32)
                self.q[l, part, x] = (self.q[l, part, x].astype(f32) + came).astype(bf16)
                self.sum_copy(l, j, "B" + key).start()
        else:
            self.await_bytes(self.rf.at[l, :, rows], self.u_sem.at[sem + 2])
            for slot in range(lo // NY, (lo + n) // NY):
                near, place = pl.ds(slot * NY, NY), pl.ds(self.z_of(slot) * NY, NY)
                total = self.q[l, near, self.xi].astype(f32)
                total += self.rf[l, 0, near].astype(f32) + self.rf[l, 1, near].astype(f32)
                scale = self.scales[l, place, self.xi]
                scale = jnp.concatenate([scale, scale], axis=2)
                old = self.s[l, place if l == 0 else near, self.rows(self.xi), self.lanes()].astype(f32)
                new = (total * scale + RESIDUAL * old).astype(bf16)
                if l == 0:
                    self.s[1, near, self.rows(self.xi), self.lanes()] = new
                else:
                    self.fin_[near] = new
            if l == 1:
                self.each_out(j, lambda slot, y: self.out_copy(slot, y).start())

    def out_copy(self, slot, y):
        return self.remote(
            self.fin_.at[slot * NY + y],
            self.s.at[2, opposite(slot) * NY + self.yi, self.rows(self.xi), self.lanes()],
            self.o_send_sem.at[0],
            self.o_sem.at[distance_of(slot)],
            {"z": self.z_of(slot), "y": y},
        )

    def each_out(self, j, do):
        lo, n = SUM_CHUNKS[1][j]
        for slot in range(lo // NY, (lo + n) // NY):
            for k in range(1 if slot == 0 else 0, NY):
                do(slot, lax.rem(self.yi + k, NY))

    def out_(self, j):
        n = SUM_CHUNKS[1][j][1]
        if j == 0:
            n -= 1
            self.s[2, self.yi, self.rows(self.xi), self.lanes()] = self.fin_[self.yi]
        self.await_bytes(self.fin_.at[pl.ds(0, n)], self.o_sem.at[j])

    def fin_copy(self, slot):
        return pltpu.make_async_copy(
            self.s.at[2, pl.ds(slot * NY, NY)],
            self.out.at[pl.ds(self.z_of(slot) * NY, NY)],
            self.l_sem.at[2],
        )

    def fin(self, j):
        lo, n = SHARE_CHUNKS[2][j]
        for slot in range(lo // NY, (lo + n) // NY):
            self.fin_copy(slot).start()

    def run(self):
        self.enter()
        for event in ORDER:
            name, rest = event[0], event[1:]
            if name == "halo":
                self.halo_copy(*rest).start()
            elif name in ("in", "out"):
                getattr(self, name + "_")(*rest)
            else:
                getattr(self, name)(*rest)
        self.await_bytes(self.w.at[:, pl.ds(0, NR - 1)], self.g_send_sem.at[0])
        self.await_bytes(self.fin_.at[pl.ds(0, NR - 1)], self.i_send_sem.at[0])
        self.await_bytes(self.s.at[:, pl.ds(0, 28)], self.s_send_sem.at[0])
        self.await_bytes(self.s.at[pl.ds(0, 2), pl.ds(0, 28)], self.u_send_sem.at[0])
        self.await_bytes(self.fin_.at[pl.ds(0, NR - 1)], self.o_send_sem.at[0])
        self.await_bytes(self.s.at[2], self.l_sem.at[2])


def kernel(*refs):
    Program(refs).run()


def per_device(
    tokens, norm_gain, up_weight, gate_weight, up_scale, gate_scale, up_taps, gate_taps,
    down_weight, down_scale,
):
    bf16, f32 = jnp.bfloat16, jnp.float32
    vmem, hbm = pl.BlockSpec(memory_space=pltpu.VMEM), pl.BlockSpec(memory_space=pl.ANY)
    dma = pltpu.SemaphoreType.DMA
    n = len(ITEMS)
    out = pl.pallas_call(
        kernel,
        out_shape=jax.ShapeDtypeStruct((NR, 64, 512), bf16),
        in_specs=[hbm] * 4 + [vmem] * 6,
        out_specs=hbm,
        scratch_shapes=[
            pltpu.VMEM((6, 64, 768), f32),
            pltpu.VMEM((2, NR, 4, 16, 128), f32),
            pltpu.VMEM((6, NR, 64, 768), bf16),
            pltpu.VMEM((3, NR, 64, 512), bf16),
            pltpu.VMEM((512, 2048), bf16),
            pltpu.VMEM((2, 520, 768), f32),
            pltpu.VMEM((2, 2, 8, 768), f32),
            pltpu.VMEM((512, 768), bf16),
            pltpu.VMEM((2, NR, 4, 16, 512), bf16),
            pltpu.VMEM((2, NR, 4, 16, 256), bf16),
            pltpu.VMEM((2, NR, 4, 16, 256), bf16),
            pltpu.VMEM((2, 2, NR // 2, 16, 256), bf16),
            pltpu.VMEM((2, 2, NR, 16, 256), bf16),
            pltpu.VMEM((NR, 16, 256), bf16),
            dma((3,)),
            dma((1,)), dma((n, 20)),
            dma((1,)), dma((1,)),
            dma((1,)), dma((SHARE_SEMS,)),
            dma((1,)), dma((SUM_SEMS,)),
            dma((2,)), dma((2,)),
            dma((1,)), dma((5,)),
            pltpu.SemaphoreType.REGULAR((5,)),
        ],
        compiler_params=pltpu.CompilerParams(
            collective_id=0, has_side_effects=True, vmem_limit_bytes=60 * 2**20
        ),
    )(
        tokens, up_weight, gate_weight, down_weight, norm_gain, up_scale, gate_scale,
        up_taps.transpose(1, 0, 2), gate_taps.transpose(1, 0, 2), down_scale,
    )
    return out.transpose(1, 0, 2).reshape(64, NR * 512)


def solution(mesh):
    torus = Mesh(mesh.devices.reshape(NZ, NY, NX, 2), ("z", "y", "x", "c"))
    ra, cb = ("z", "y"), ("x", "c")
    placed = (
        P(ra, None),
        P(),
        P(None, ra, cb),
        P(None, ra, cb),
        P(None, cb),
        P(None, cb),
        P(None, None, cb),
        P(None, None, cb),
        P(None, ra, cb),
        P(),
    )
    return jax.shard_map(
        per_device, mesh=torus, in_specs=placed, out_specs=P(ra, None), check_vma=False
    )
```

```python
import jax
import jax.numpy as jnp
from jax import lax
from jax.experimental import pallas as pl
from jax.experimental.pallas import tpu as pltpu
from jax.sharding import Mesh
from jax.sharding import PartitionSpec as P

MESH = pl.DeviceIdType.MESH
EPS = 1e-06
RESIDUAL = 0.5
NZ, NY, NX = 8, 4, 4
NR = NZ * NY

ITEMS = [(0, 0, 256, 768), (1, 0, 384, 768), (2, 0, 256, 768), (3, 0, 256, 768), (4, 0, 384, 768), (5, 0, 256, 768)]
PAIR_KEYS = ("Ay1", "Ay2", "Az1", "Az2", "Az3", "Az4", "Bz1", "Bz2", "Bz3", "Bz4")
KEY = {k: i for i, k in enumerate(PAIR_KEYS)}
for _k, _name in enumerate(("By1", "By2")):
    for _distance in range(5):
        KEY[_name, _distance] = 10 + 5 * _k + _distance

NEAR = ((0, 4), (4, 8), (12, 8), (20, 8), (28, 4))
HALVES = ((0, 16), (16, 16))
FIRST = ((0, 8), (8, 8), (16, 8), (24, 8))
SHARE_CHUNKS = (HALVES, FIRST, NEAR)
SUM_CHUNKS = (FIRST, NEAR)
SHARE_SEMS = 3 * 13
SUM_SEMS = 3 * 10


def offset(slot):
    return (slot + 1) // 2 * (2 * (slot % 2) - 1)


def slots_at(distance):
    return (0,) if distance == 0 else (7,) if distance == 4 else (2 * distance - 1, 2 * distance)


def distance_of(slot):
    return (slot + 1) // 2


def opposite(slot):
    return slot if slot in (0, 7) else slot + 1 if slot % 2 else slot - 1


ORDER = [
    ("A", 2, 0), ("A", 0, 0), ("B", 0, 0), ("B", 1, 0), ("A", 1, 0), ("B", 4, 0), ("know", 0),
    ("B", 0, 1), ("A", 0, 1), ("B", 2, 0), ("know", 1), ("know", 2), ("know", 3), ("B", 1, 1),
    ("A", 4, 0), ("B", 3, 0), ("B", 0, 2), ("know", 4), ("A", 1, 1), ("know", 5), ("B", 1, 2),
    ("in", 0), ("B", 1, 3), ("A", 2, 1), ("B", 2, 1), ("A", 0, 2), ("A", 1, 2), ("in", 1),
    ("B", 0, 3), ("A", 0, 3), ("share", 0, 0, 0), ("A", 1, 3), ("C", 1, 3), ("B", 0, 4),
    ("C", 0, 0), ("B", 1, 4), ("A", 0, 4), ("A", 3, 0), ("C", 1, 1), ("share", 0, 1, 0),
    ("B", 4, 1), ("B", 3, 1), ("A", 1, 4), ("C", 0, 4), ("scale",), ("C", 2, 0), ("C", 0, 2),
    ("C", 1, 2), ("A", 3, 1), ("C", 1, 4), ("C", 0, 3), ("A", 2, 2), ("share", 0, 1, 1),
    ("A", 1, 5), ("C", 1, 0), ("E", 2, 0), ("E", 0, 2), ("B", 2, 2), ("C", 0, 1), ("A", 4, 1),
    ("A", 0, 5), ("E", 0, 3), ("A", 2, 3), ("B", 2, 3), ("B", 3, 2), ("E", 1, 1),
    ("share", 0, 1, 2), ("share", 0, 1, 3), ("A", 3, 2), ("share", 0, 0, 1), ("E", 1, 0),
    ("E", 1, 4), ("B", 5, 0), ("A", 0, 6), ("share", 0, 0, 2), ("share", 0, 0, 3), ("C", 2, 3),
    ("A", 2, 4), ("E", 1, 2), ("E", 0, 4), ("E", 0, 0), ("E", 1, 3), ("B", 3, 3), ("prep", 0),
    ("A", 4, 2), ("A", 1, 6), ("E", 0, 1), ("ug", 0, 0), ("ug", 0, 1), ("halo", 0, 1), ("ug", 0, 2),
    ("halo", 0, 2), ("halo", 0, 0), ("C", 2, 2), ("C", 2, 1), ("B", 2, 4), ("B", 4, 2), ("conv", 0),
    ("E", 2, 2), ("A", 2, 5), ("E", 2, 3), ("down", 0, 2), ("sum", 0, 2, 0), ("A", 4, 3),
    ("A", 5, 0), ("A", 3, 3), ("E", 2, 1), ("down", 0, 0), ("sum", 0, 0, 0), ("B", 4, 3),
    ("C", 4, 0), ("down", 0, 1), ("sum", 0, 1, 0), ("sum", 0, 2, 1), ("C", 2, 4), ("sum", 0, 0, 1),
    ("B", 3, 4), ("A", 2, 6), ("C", 3, 1), ("A", 5, 1), ("C", 3, 2), ("sum", 0, 1, 1),
    ("sum", 0, 2, 2), ("B", 5, 1), ("C", 3, 0), ("sum", 0, 0, 2), ("E", 4, 0), ("E", 2, 4),
    ("down", 0, 3), ("sum", 0, 3, 0), ("sum", 0, 1, 2), ("A", 3, 4), ("C", 4, 3), ("sum", 0, 3, 1),
    ("sum", 0, 0, 3), ("A", 4, 4), ("A", 5, 2), ("share", 1, 0, 0), ("C", 3, 4), ("sum", 0, 2, 3),
    ("share", 1, 2, 0), ("sum", 0, 3, 2), ("B", 4, 4), ("B", 5, 2), ("share", 1, 0, 1), ("C", 4, 1),
    ("sum", 0, 1, 3), ("C", 4, 2), ("share", 1, 1, 0), ("sum", 0, 3, 3), ("share", 1, 3, 0),
    ("E", 3, 0), ("share", 1, 0, 2), ("share", 1, 1, 1), ("share", 1, 0, 3), ("E", 3, 4),
    ("C", 4, 4), ("E", 3, 1), ("C", 3, 3), ("share", 1, 2, 1), ("A", 3, 5), ("share", 1, 3, 1),
    ("A", 4, 5), ("C", 5, 2), ("E", 4, 3), ("C", 5, 0), ("A", 5, 3), ("share", 1, 2, 2),
    ("share", 1, 1, 2), ("B", 5, 3), ("share", 1, 3, 2), ("C", 5, 1), ("E", 4, 2), ("E", 3, 2),
    ("share", 1, 1, 3), ("share", 1, 2, 3), ("A", 3, 6), ("E", 4, 1), ("E", 4, 4),
    ("share", 1, 3, 3), ("prep", 1), ("E", 3, 3), ("A", 4, 6), ("ug", 1, 0), ("halo", 1, 0),
    ("ug", 1, 1), ("halo", 1, 1), ("ug", 1, 2), ("halo", 1, 2), ("A", 5, 4), ("B", 5, 4),
    ("C", 5, 3), ("E", 5, 1), ("E", 5, 0), ("conv", 1), ("down", 1, 0), ("sum", 1, 0, 0),
    ("down", 1, 1), ("sum", 1, 1, 0), ("E", 5, 2), ("E", 5, 3), ("A", 5, 5), ("down", 1, 3),
    ("sum", 1, 3, 0), ("C", 5, 4), ("sum", 1, 0, 1), ("sum", 1, 1, 1), ("down", 1, 2),
    ("sum", 1, 3, 1), ("sum", 1, 2, 0), ("E", 5, 4), ("sum", 1, 0, 2), ("sum", 1, 2, 1),
    ("A", 5, 6), ("down", 1, 4), ("sum", 1, 4, 0), ("sum", 1, 3, 2), ("sum", 1, 0, 3),
    ("sum", 1, 4, 1), ("sum", 1, 2, 2), ("sum", 1, 1, 2), ("sum", 1, 3, 3), ("sum", 1, 4, 2),
    ("sum", 1, 2, 3), ("sum", 1, 1, 3), ("sum", 1, 4, 3), ("out", 0), ("share", 2, 0, 0),
    ("out", 3), ("share", 2, 3, 0), ("out", 2), ("share", 2, 2, 0), ("share", 2, 0, 1), ("out", 1),
    ("share", 2, 1, 0), ("share", 2, 3, 1), ("out", 4), ("share", 2, 4, 0), ("share", 2, 1, 1),
    ("share", 2, 2, 1), ("share", 2, 0, 2), ("share", 2, 4, 1), ("share", 2, 3, 2),
    ("share", 2, 3, 3), ("share", 2, 1, 2), ("share", 2, 0, 3), ("share", 2, 2, 2),
    ("share", 2, 4, 2), ("fin", 0), ("share", 2, 1, 3), ("share", 2, 2, 3), ("fin", 3), ("fin", 1),
    ("fin", 2), ("share", 2, 4, 3), ("fin", 4),
]


class Program:
    def __init__(self, refs):
        (
            self.tok, self.wu, self.wg, self.wd, *small, self.out,
            self.gain, self.us, self.gs, self.ut, self.gt, self.ds, self.stage, self.scales,
            self.w, self.s, self.x, self.pre, self.halo, self.hid, self.part, self.rd, self.q,
            self.rh, self.rf, self.fin_,
            self.l_sem, self.g_send_sem, self.g_sem, self.i_send_sem, self.i_sem,
            self.s_send_sem, self.s_sem, self.u_send_sem, self.u_sem, self.h_send_sem, self.h_sem,
            self.o_send_sem, self.o_sem, self.know_sem,
        ) = refs
        self.zi, self.yi = lax.axis_index("z"), lax.axis_index("y")
        self.xi, self.ci = lax.axis_index("x"), lax.axis_index("c")
        self.ri = self.zi * NY + self.yi
        self.w_copies = [
            pltpu.make_async_copy((self.wu, self.wg, self.wd)[m % 3].at[m // 3], self.stage.at[m], self.l_sem.at[0])
            for m in range(6)
        ]

        self.small_copies = [
            pltpu.make_async_copy(a, b, self.l_sem.at[2 + k])
            for k, (a, b) in enumerate(
                zip(small, (self.gain, self.us, self.gs, self.ut, self.gt, self.ds), strict=True)
            )
        ]

    def z_of(self, slot):
        return lax.rem(self.zi + offset(slot) + NZ, NZ)

    def enter(self):
        for c in self.w_copies + self.small_copies:
            c.start()
        barrier = pltpu.get_barrier_semaphore()

        def tell(to):
            pl.semaphore_signal(barrier, inc=1, device_id=to, device_id_type=MESH)

        tell(self.step_to("c", "p"))
        for link in "xyz":
            for d in "pm":
                tell(self.step_to(link, d))
        pltpu.make_async_copy(self.stage, self.stage, self.l_sem.at[0]).wait()
        for m in range(6):
            self.w[m, self.ri] = self.stage[m].astype(jnp.bfloat16)
        pl.semaphore_wait(barrier, 7)

    def know(self, k):
        if k > 0:
            pl.semaphore_wait(self.know_sem.at[k - 1], 2)
        if k < 5:
            for d in "pm":
                pl.semaphore_signal(
                    self.know_sem.at[k], inc=1, device_id=self.step_to("y" if k == 0 else "z", d),
                    device_id_type=MESH,
                )

    def gather_region(self, i, key, d, slot):
        m, c0, c1, c2 = ITEMS[i]
        sign = 1 if d == "p" else -1
        hop = int(key[2])
        back = hop - 1
        first, second = pl.ds(c0, c1 - c0), pl.ds(c1, c2 - c1)
        z = lax.rem(self.zi - sign * back + NZ, NZ)
        y = lax.rem(self.yi - sign * back + NY, NY)
        half = pl.ds(0 if d == "p" else 32, 32)
        w = self.w.at[m]
        if key[:2] == "Ay":
            return w.at[self.zi * NY + y, half if hop == 2 else slice(None), first]
        if key[:2] == "Az":
            if hop == 4:
                return w.at[pl.ds(z * NY + (0 if d == "p" else 2), 2), :, first]
            return w.at[pl.ds(z * NY, NY), :, first]
        if key[:2] == "Bz":
            return w.at[z * NY + self.yi, half if hop == 4 else slice(None), second]
        return w.at[self.z_of(slot) * NY + y, half if hop == 2 else slice(None), second]

    def step_to(self, link, d):
        if link == "z":
            return {"z": lax.rem(self.zi + (1 if d == "p" else NZ - 1), NZ)}
        if link == "y":
            return {"y": lax.rem(self.yi + (1 if d == "p" else NY - 1), NY)}
        if link == "x":
            return {"x": lax.rem(self.xi + (1 if d == "p" else NX - 1), NX)}
        return {"c": 1 - self.ci}

    @staticmethod
    def remote(src, dst, send, recv, to):
        return pltpu.make_async_remote_copy(
            src_ref=src, dst_ref=dst, send_sem=send, recv_sem=recv, device_id=to, device_id_type=MESH
        )

    def g_copy(self, i, key, d, slot=None):
        region = self.gather_region(i, key, d, slot)
        k = KEY[key] if slot is None else KEY[key, distance_of(slot)]
        return self.remote(
            region, region, self.g_send_sem.at[0], self.g_sem.at[i, k], self.step_to(key[1], d)
        )

    def g_send(self, i, key, slots=(None,)):
        for slot in slots:
            for d in "pm":
                self.g_copy(i, key, d, slot).start()

    def await_bytes(self, like, sem):
        pltpu.make_async_copy(like, like, sem).wait()

    def g_wait(self, i, key, distance=None):
        m, c0, c1, c2 = ITEMS[i]
        cols = pl.ds(c0, c1 - c0) if key[0] == "A" else pl.ds(c1, c2 - c1)
        shards = {"Ay1": 2, "Ay2": 1, "Az4": 4, "Bz4": 1}.get(key, 8 if key[:2] == "Az" else 2)
        k = KEY[key] if distance is None else KEY[key, distance]
        if distance is not None:
            shards = len(slots_at(distance)) * (2 if key == "By1" else 1)
        self.await_bytes(self.w.at[m, pl.ds(0, shards), :, cols], self.g_sem.at[i, k])

    def g_forward(self, i, came, goes):
        self.g_wait(i, came)
        self.g_send(i, goes)

    def A(self, i, st):
        if st == 0:
            self.g_send(i, "Ay1")
        elif st == 1:
            self.g_forward(i, "Ay1", "Ay2")
        elif st == 2:
            self.g_wait(i, "Ay2")
            self.g_send(i, "Az1")
        elif st < 6:
            self.g_forward(i, f"Az{st - 2}", f"Az{st - 1}")
        else:
            self.g_wait(i, "Az4")

    def B(self, i, st):
        if st == 0:
            self.g_send(i, "Bz1")
        elif st < 4:
            self.g_forward(i, f"Bz{st}", f"Bz{st + 1}")
        else:
            self.g_wait(i, "Bz4")
        self.g_send(i, "By1", slots_at(st))

    def C(self, i, distance):
        self.g_wait(i, "By1", distance)
        self.g_send(i, "By2", slots_at(distance))

    def E(self, i, distance):
        self.g_wait(i, "By2", distance)

    def lanes(self, own=True):
        c = self.ci if own else 1 - self.ci
        return pl.ds(pl.multiple_of(c * 256, 256), 256)

    def rows(self, x):
        return pl.ds(pl.multiple_of(x * 16, 16), 16)

    def in_own(self):
        cols = pl.ds(pl.multiple_of(self.ri * 512 + self.ci * 256, 256), 256)
        rows = pl.ds(pl.multiple_of(self.xi * 16, 16), 16)
        return pltpu.make_async_copy(
            self.tok.at[rows, cols], self.s.at[0, self.ri, self.rows(self.xi), self.lanes()], self.l_sem.at[1]
        )

    def in_copy(self, other):
        cols = pl.ds(pl.multiple_of(other * 512 + self.ci * 256, 256), 256)
        rows = pl.ds(pl.multiple_of(self.xi * 16, 16), 16)
        return self.remote(
            self.tok.at[rows, cols],
            self.s.at[0, self.ri, self.rows(self.xi), self.lanes()],
            self.i_send_sem.at[0],
            self.i_sem.at[0],
            {"z": other // NY, "y": lax.rem(other, NY)},
        )

    def each_other(self, do):
        def body(k, carry):
            do(lax.rem(self.ri + k, NR))
            return carry

        lax.fori_loop(1, NR, body, 0)

    def in_(self, st):
        if st == 0:
            self.in_own().start()
            self.each_other(lambda o: self.in_copy(o).start())
        else:
            self.in_own().wait()
            self.await_bytes(self.fin_.at[pl.ds(0, NR - 1)], self.i_sem.at[0])

    def share_copy(self, which, j, key):
        lo, n = SHARE_CHUNKS[which][j]
        sem = self.s_sem.at[(4 * which + j) * 3 + {"X1": 0, "X2": 1}.get(key[:2], 2)]
        if key[0] == "X":
            sign = 1 if key[2] == "p" else -1
            hop = int(key[1])
            x = lax.rem(self.xi - sign * (hop - 1) + NX, NX)
            if hop == 2:
                n = n // 2
                lo += 0 if key[2] == "p" else n
            to = self.step_to("x", key[2])
        else:
            x = lax.rem(self.xi + {"D0": 0, "D1": NX - 1, "D2": 1, "D3": 2}[key], NX)
            to = self.step_to("c", "p")
        region = self.s.at[which, pl.ds(lo, n), self.rows(x), self.lanes()]
        return self.remote(region, region, self.s_send_sem.at[0], sem, to)

    def share(self, which, j, st):
        lo, n = SHARE_CHUNKS[which][j]
        sem = (4 * which + j) * 3

        def start(*keys):
            for k in keys:
                self.share_copy(which, j, k).start()

        def arrived(quarters, k):
            like = self.s.at[which, pl.ds(lo, n), pl.ds(0, 16 * quarters), self.lanes()]
            self.await_bytes(like, self.s_sem.at[sem + k])

        if st == 0:
            start("X1p", "X1m", "D0")
        elif st == 1:
            arrived(2, 0)
            start("X2p", "X2m", "D1", "D2")
        elif st == 2:
            arrived(1, 1)
            start("D3")
        else:
            arrived(4, 2)

    def prep(self, l):
        def body(k, acc):
            block = self.s[l, pl.ds(k * 4, 4)].reshape(256, 512)
            t = block.T.astype(jnp.float32)
            z = k if l == 0 else self.z_of(k)
            cols = pl.ds(pl.multiple_of(z * 256, 256), 256)
            self.x[:, cols] = (t * self.gain[l : l + 1, cols]).astype(jnp.bfloat16)
            sq = t * t
            return acc + sq[:, :128] + sq[:, 128:]

        acc = lax.fori_loop(0, 8, body, jnp.zeros((512, 128), jnp.float32))
        mean = jnp.sum(acc, axis=1, keepdims=True) * (1.0 / 2048)
        self.inverse = lax.rsqrt(mean + EPS)

    def ug(self, l, n):
        cols = slice(n * 256, n * 256 + 256)
        for k, scale in ((0, self.us), (1, self.gs)):
            w = self.w[3 * l + k, :, :, cols].reshape(2048, 256)
            raw = jnp.dot(self.x[...], w, preferred_element_type=jnp.float32)
            self.pre[k, 8:520, cols] = raw * self.inverse * scale[l : l + 1, cols]

    def halo_copy(self, l, n):
        cols = pl.ds(n * 256, 256)
        wrap = jnp.where(self.yi == NY - 1, 1, 0)
        to = {"z": lax.rem(self.zi + wrap, NZ), "y": lax.rem(self.yi + 1, NY)}
        return self.remote(
            self.pre.at[:, pl.ds(512, 8), cols], self.halo.at[l, :, :, cols],
            self.h_send_sem.at[l], self.h_sem.at[l], to,
        )

    def conv(self, l):
        self.await_bytes(self.halo.at[l], self.h_sem.at[l])
        first = self.ri == 0
        for n in range(6):
            cols = slice(n * 128, n * 128 + 128)
            both = []
            for k, taps in ((0, self.ut), (1, self.gt)):
                before = self.halo[l, k, :, cols]
                self.pre[k, 0:8, cols] = jnp.where(first, jnp.zeros_like(before), before)
                total = taps[0, l : l + 1, cols] * self.pre[k, 6:518, cols]
                total += taps[1, l : l + 1, cols] * self.pre[k, 7:519, cols]
                total += taps[2, l : l + 1, cols] * self.pre[k, 8:520, cols]
                both.append(total)
            up, gate = both
            self.hid[:, cols] = (gate / (1.0 + jnp.exp(-gate)) * up).astype(jnp.bfloat16)
        self.await_bytes(self.halo.at[l], self.h_send_sem.at[l])

    def scale(self):
        def body(k, carry):
            cols = pl.ds(pl.multiple_of(k * 128, 128), 128)
            for l in range(2):
                row = jnp.broadcast_to(self.ds[l : l + 1, cols], (128, 128))
                self.scales[l, pl.ds(k * 2, 2)] = row.T.reshape(2, 4, 16, 128)
            return carry

        lax.fori_loop(0, 16, body, 0)

    def down(self, l, j):
        lo, n = SUM_CHUNKS[l][j]
        width = 2 if n > NY else 1

        def body(k, carry):
            slot = lo // NY + width * k
            w = jnp.concatenate(
                [
                    self.w[3 * l + 2, pl.ds(self.z_of(slot + i) * NY, NY)].reshape(256, 768)
                    for i in range(width)
                ]
            )
            part = lax.dot_general(
                w, self.hid[...], (((1,), (1,)), ((), ())), preferred_element_type=jnp.float32
            ).astype(jnp.bfloat16)
            self.part[l, pl.ds(slot * NY, NY * width)] = part.reshape(NY * width, 4, 16, 512)
            return carry

        lax.fori_loop(0, n // (NY * width), body, 0)

    def sum_copy(self, l, j, key):
        lo, n = SUM_CHUNKS[l][j]
        h = n // 2
        k = (4 * l + j) * 3 + "DAB".index(key[0])
        sems = (self.u_send_sem.at[0], self.u_sem.at[k])
        if key == "D":
            return self.remote(
                self.part.at[l, pl.ds(lo, n), :, :, self.lanes(False)],
                self.rd.at[l, pl.ds(lo, n)], *sems, self.step_to("c", "p"),
            )
        d = key[1]
        if key[0] == "A":
            first = lo + (0 if d == "p" else h)
            return self.remote(
                self.q.at[l, pl.ds(first, h), lax.rem(self.xi + 2, NX)],
                self.rh.at[l, 0 if d == "p" else 1, pl.ds(lo // 2, h)], *sems, self.step_to("x", d),
            )
        return self.remote(
            self.q.at[l, pl.ds(lo, n), lax.rem(self.xi + (1 if d == "p" else NX - 1), NX)],
            self.rf.at[l, 0 if d == "p" else 1, pl.ds(lo, n)], *sems, self.step_to("x", d),
        )

    def sum(self, l, j, st):
        lo, n = SUM_CHUNKS[l][j]
        h = n // 2
        f32, bf16 = jnp.float32, jnp.bfloat16
        rows = pl.ds(lo, n)
        sem = (4 * l + j) * 3
        if st == 0:
            self.sum_copy(l, j, "D").start()
        elif st == 1:
            self.await_bytes(self.rd.at[l, rows], self.u_sem.at[sem])
            mine = self.part[l, rows, :, :, self.lanes()].astype(f32)
            self.q[l, rows] = (mine + self.rd[l, rows].astype(f32)).astype(bf16)
            self.sum_copy(l, j, "Ap").start()
            self.sum_copy(l, j, "Am").start()
        elif st == 2:
            self.await_bytes(self.rh.at[l, :, pl.ds(lo // 2, h)], self.u_sem.at[sem + 1])
            for d, key in ((1, "p"), (-1, "m")):
                x = lax.rem(self.xi + d + NX, NX)
                part = pl.ds(lo + (0 if key == "p" else h), h)
                came = self.rh[l, 0 if key == "p" else 1, pl.ds(lo // 2, h)].astype(f32)
                self.q[l, part, x] = (self.q[l, part, x].astype(f32) + came).astype(bf16)
                self.sum_copy(l, j, "B" + key).start()
        else:
            self.await_bytes(self.rf.at[l, :, rows], self.u_sem.at[sem + 2])
            for slot in range(lo // NY, (lo + n) // NY):
                near, place = pl.ds(slot * NY, NY), pl.ds(self.z_of(slot) * NY, NY)
                total = self.q[l, near, self.xi].astype(f32)
                total += self.rf[l, 0, near].astype(f32) + self.rf[l, 1, near].astype(f32)
                scale = self.scales[l, place, self.xi]
                scale = jnp.concatenate([scale, scale], axis=2)
                old = self.s[l, place if l == 0 else near, self.rows(self.xi), self.lanes()].astype(f32)
                new = (total * scale + RESIDUAL * old).astype(bf16)
                if l == 0:
                    self.s[1, near, self.rows(self.xi), self.lanes()] = new
                else:
                    self.fin_[near] = new
            if l == 1:
                self.each_out(j, lambda slot, y: self.out_copy(slot, y).start())

    def out_copy(self, slot, y):
        return self.remote(
            self.fin_.at[slot * NY + y],
            self.s.at[2, opposite(slot) * NY + self.yi, self.rows(self.xi), self.lanes()],
            self.o_send_sem.at[0],
            self.o_sem.at[distance_of(slot)],
            {"z": self.z_of(slot), "y": y},
        )

    def each_out(self, j, do):
        lo, n = SUM_CHUNKS[1][j]
        for slot in range(lo // NY, (lo + n) // NY):
            for k in range(1 if slot == 0 else 0, NY):
                do(slot, lax.rem(self.yi + k, NY))

    def out_(self, j):
        n = SUM_CHUNKS[1][j][1]
        if j == 0:
            n -= 1
            self.s[2, self.yi, self.rows(self.xi), self.lanes()] = self.fin_[self.yi]
        self.await_bytes(self.fin_.at[pl.ds(0, n)], self.o_sem.at[j])

    def fin(self, j):
        lo, n = SHARE_CHUNKS[2][j]
        for slot in range(lo // NY, (lo + n) // NY):
            self.out[pl.ds(self.z_of(slot) * NY, NY)] = self.s[2, pl.ds(slot * NY, NY)]

    def run(self):
        self.enter()
        for event in ORDER:
            name, rest = event[0], event[1:]
            if self.small_copies and name in ("scale", "prep"):
                for c in self.small_copies:
                    c.wait()
                self.small_copies = []
            if name == "halo":
                self.halo_copy(*rest).start()
            elif name in ("in", "out"):
                getattr(self, name + "_")(*rest)
            else:
                getattr(self, name)(*rest)
        self.await_bytes(self.w.at[:, pl.ds(0, NR - 1)], self.g_send_sem.at[0])
        self.await_bytes(self.fin_.at[pl.ds(0, NR - 1)], self.i_send_sem.at[0])
        self.await_bytes(self.s.at[:, pl.ds(0, 28)], self.s_send_sem.at[0])
        self.await_bytes(self.s.at[pl.ds(0, 2), pl.ds(0, 28)], self.u_send_sem.at[0])
        self.await_bytes(self.fin_.at[pl.ds(0, NR - 1)], self.o_send_sem.at[0])


def kernel(*refs):
    Program(refs).run()


def per_device(
    tokens, norm_gain, up_weight, gate_weight, up_scale, gate_scale, up_taps, gate_taps,
    down_weight, down_scale,
):
    bf16, f32 = jnp.bfloat16, jnp.float32
    hbm = pl.BlockSpec(memory_space=pltpu.HBM)
    dma = pltpu.SemaphoreType.DMA
    n = len(ITEMS)
    arrays = (
        tokens, up_weight, gate_weight, down_weight, norm_gain, up_scale, gate_scale,
        up_taps.transpose(1, 0, 2), gate_taps.transpose(1, 0, 2), down_scale,
    )
    arrays = [pltpu.with_memory_space_constraint(a, pltpu.HBM) for a in arrays]
    out = pl.pallas_call(
        kernel,
        out_shape=jax.ShapeDtypeStruct((NR, 64, 512), bf16),
        in_specs=[hbm] * 10,
        out_specs=pl.BlockSpec(memory_space=pltpu.VMEM),
        scratch_shapes=[
            pltpu.VMEM((2, 2048), f32),
            pltpu.VMEM((2, 768), f32),
            pltpu.VMEM((2, 768), f32),
            pltpu.VMEM((3, 2, 768), f32),
            pltpu.VMEM((3, 2, 768), f32),
            pltpu.VMEM((2, 2048), f32),
            pltpu.VMEM((6, 64, 768), f32),
            pltpu.VMEM((2, NR, 4, 16, 128), f32),
            pltpu.VMEM((6, NR, 64, 768), bf16),
            pltpu.VMEM((3, NR, 64, 512), bf16),
            pltpu.VMEM((512, 2048), bf16),
            pltpu.VMEM((2, 520, 768), f32),
            pltpu.VMEM((2, 2, 8, 768), f32),
            pltpu.VMEM((512, 768), bf16),
            pltpu.VMEM((2, NR, 4, 16, 512), bf16),
            pltpu.VMEM((2, NR, 4, 16, 256), bf16),
            pltpu.VMEM((2, NR, 4, 16, 256), bf16),
            pltpu.VMEM((2, 2, NR // 2, 16, 256), bf16),
            pltpu.VMEM((2, 2, NR, 16, 256), bf16),
            pltpu.VMEM((NR, 16, 256), bf16),
            dma((8,)),
            dma((1,)), dma((n, 20)),
            dma((1,)), dma((1,)),
            dma((1,)), dma((SHARE_SEMS,)),
            dma((1,)), dma((SUM_SEMS,)),
            dma((2,)), dma((2,)),
            dma((1,)), dma((5,)),
            pltpu.SemaphoreType.REGULAR((5,)),
        ],
        compiler_params=pltpu.CompilerParams(
            collective_id=0, has_side_effects=True, vmem_limit_bytes=50 * 2**20
        ),
    )(*arrays)
    return out.transpose(1, 0, 2).reshape(64, NR * 512)


def solution(mesh):
    torus = Mesh(mesh.devices.reshape(NZ, NY, NX, 2), ("z", "y", "x", "c"))
    ra, cb = ("z", "y"), ("x", "c")
    placed = (
        P(ra, None),
        P(),
        P(None, ra, cb),
        P(None, ra, cb),
        P(None, cb),
        P(None, cb),
        P(None, None, cb),
        P(None, None, cb),
        P(None, ra, cb),
        P(),
    )
    return jax.shard_map(
        per_device, mesh=torus, in_specs=placed, out_specs=P(ra, None), check_vma=False
    )
```

```python
import jax
import jax.numpy as jnp
from jax import lax
from jax.experimental import pallas as pl
from jax.experimental.pallas import tpu as pltpu
from jax.sharding import Mesh
from jax.sharding import PartitionSpec as P

MESH = pl.DeviceIdType.MESH
EPS = 1e-06
RESIDUAL = 0.5
NZ, NY, NX = 8, 4, 4
NR = NZ * NY

ITEMS = [(0, 0, 256, 768), (1, 0, 384, 768), (2, 0, 256, 768), (3, 0, 256, 768), (4, 0, 384, 768), (5, 0, 256, 768)]
PAIR_KEYS = ("Ay1", "Ay2", "Az1", "Az2", "Az3", "Az4", "Bz1", "Bz2", "Bz3", "Bz4")
KEY = {k: i for i, k in enumerate(PAIR_KEYS)}
for _k, _name in enumerate(("By1", "By2")):
    for _distance in range(5):
        KEY[_name, _distance] = 10 + 5 * _k + _distance

NEAR = ((0, 4), (4, 8), (12, 8), (20, 8), (28, 4))
HALVES = ((0, 16), (16, 16))
FIRST = ((0, 8), (8, 8), (16, 8), (24, 8))
SHARE_CHUNKS = (HALVES, FIRST, NEAR)
SUM_CHUNKS = (FIRST, NEAR)
SHARE_SEMS = 3 * 13
SUM_SEMS = 3 * 10


def offset(slot):
    return (slot + 1) // 2 * (2 * (slot % 2) - 1)


def slots_at(distance):
    return (0,) if distance == 0 else (7,) if distance == 4 else (2 * distance - 1, 2 * distance)


def distance_of(slot):
    return (slot + 1) // 2


def opposite(slot):
    return slot if slot in (0, 7) else slot + 1 if slot % 2 else slot - 1


ORDER = [
    ("A", 2, 0), ("B", 1, 0), ("A", 0, 0), ("B", 2, 0), ("B", 0, 0), ("A", 2, 1), ("B", 4, 0),
    ("B", 1, 1), ("know", 0), ("A", 1, 0), ("A", 0, 1), ("B", 2, 1), ("know", 1), ("A", 5, 0),
    ("B", 0, 1), ("know", 2), ("A", 2, 2), ("know", 3), ("B", 1, 2), ("A", 0, 2), ("A", 1, 1),
    ("A", 3, 0), ("know", 4), ("B", 2, 2), ("B", 0, 2), ("B", 4, 1), ("know", 5), ("A", 4, 0),
    ("C", 0, 0), ("in", 0), ("A", 1, 2), ("B", 0, 3), ("A", 0, 3), ("A", 2, 3), ("A", 5, 1),
    ("C", 2, 1), ("B", 2, 3), ("C", 0, 2), ("in", 1), ("B", 1, 3), ("share", 0, 0, 0), ("A", 1, 3),
    ("A", 0, 4), ("B", 1, 4), ("C", 0, 3), ("B", 4, 2), ("A", 2, 4), ("A", 1, 4),
    ("share", 0, 0, 1), ("A", 3, 1), ("C", 4, 0), ("share", 0, 1, 0), ("C", 1, 1), ("B", 3, 0),
    ("C", 1, 3), ("scale",), ("B", 0, 4), ("A", 0, 5), ("share", 0, 1, 1), ("share", 0, 0, 2),
    ("E", 0, 3), ("E", 2, 1), ("C", 0, 1), ("A", 1, 5), ("A", 2, 5), ("share", 0, 0, 3),
    ("E", 4, 0), ("B", 4, 3), ("C", 0, 4), ("share", 0, 1, 2), ("A", 3, 2), ("E", 0, 0),
    ("C", 1, 0), ("C", 1, 2), ("share", 0, 1, 3), ("prep", 0), ("C", 1, 4), ("B", 5, 0),
    ("B", 3, 1), ("E", 0, 2), ("C", 2, 2), ("E", 0, 1), ("B", 2, 4), ("C", 4, 3), ("A", 4, 1),
    ("E", 1, 3), ("A", 1, 6), ("E", 1, 1), ("A", 5, 2), ("E", 1, 2), ("E", 1, 0), ("E", 0, 4),
    ("E", 1, 4), ("A", 0, 6), ("ug", 0, 0), ("halo", 0, 0), ("ug", 0, 1), ("A", 3, 3), ("C", 2, 0),
    ("halo", 0, 1), ("ug", 0, 2), ("A", 2, 6), ("halo", 0, 2), ("C", 2, 3), ("C", 2, 4),
    ("B", 3, 2), ("A", 4, 2), ("C", 4, 1), ("B", 5, 1), ("conv", 0), ("E", 2, 3), ("B", 3, 3),
    ("E", 2, 4), ("down", 0, 3), ("sum", 0, 3, 0), ("E", 2, 2), ("down", 0, 1), ("down", 0, 2),
    ("sum", 0, 2, 0), ("sum", 0, 1, 0), ("sum", 0, 3, 1), ("E", 2, 0), ("down", 0, 0),
    ("sum", 0, 0, 0), ("A", 4, 3), ("sum", 0, 2, 1), ("sum", 0, 1, 1), ("C", 3, 1), ("E", 4, 3),
    ("A", 3, 4), ("sum", 0, 0, 1), ("B", 5, 2), ("sum", 0, 3, 2), ("sum", 0, 2, 2), ("B", 3, 4),
    ("C", 5, 1), ("sum", 0, 1, 2), ("sum", 0, 0, 2), ("sum", 0, 2, 3), ("share", 1, 2, 0),
    ("B", 4, 4), ("A", 4, 4), ("sum", 0, 1, 3), ("share", 1, 1, 0), ("C", 3, 3), ("C", 3, 0),
    ("sum", 0, 0, 3), ("share", 1, 0, 0), ("A", 3, 5), ("C", 5, 0), ("E", 5, 1), ("sum", 0, 3, 3),
    ("share", 1, 3, 0), ("C", 3, 4), ("share", 1, 2, 1), ("A", 5, 3), ("C", 3, 2), ("C", 4, 4),
    ("share", 1, 1, 1), ("C", 4, 2), ("B", 5, 3), ("share", 1, 0, 1), ("share", 1, 3, 1),
    ("share", 1, 2, 2), ("E", 3, 4), ("share", 1, 1, 2), ("A", 4, 5), ("E", 4, 1),
    ("share", 1, 0, 2), ("E", 3, 0), ("share", 1, 2, 3), ("E", 3, 1), ("share", 1, 3, 2),
    ("A", 3, 6), ("C", 5, 2), ("share", 1, 1, 3), ("E", 3, 2), ("A", 5, 4), ("E", 5, 0),
    ("E", 4, 2), ("share", 1, 0, 3), ("E", 3, 3), ("B", 5, 4), ("E", 4, 4), ("share", 1, 3, 3),
    ("prep", 1), ("A", 4, 6), ("ug", 1, 0), ("ug", 1, 1), ("halo", 1, 1), ("halo", 1, 0),
    ("ug", 1, 2), ("halo", 1, 2), ("E", 5, 2), ("C", 5, 4), ("A", 5, 5), ("C", 5, 3), ("conv", 1),
    ("down", 1, 1), ("sum", 1, 1, 0), ("E", 5, 3), ("down", 1, 3), ("sum", 1, 3, 0), ("down", 1, 2),
    ("sum", 1, 1, 1), ("sum", 1, 2, 0), ("down", 1, 0), ("sum", 1, 0, 0), ("sum", 1, 3, 1),
    ("A", 5, 6), ("sum", 1, 2, 1), ("sum", 1, 0, 1), ("sum", 1, 1, 2), ("E", 5, 4), ("down", 1, 4),
    ("sum", 1, 4, 0), ("sum", 1, 3, 2), ("sum", 1, 4, 1), ("sum", 1, 0, 2), ("sum", 1, 2, 2),
    ("sum", 1, 1, 3), ("sum", 1, 3, 3), ("sum", 1, 4, 2), ("sum", 1, 0, 3), ("sum", 1, 2, 3),
    ("sum", 1, 4, 3), ("out", 1), ("share", 2, 1, 0), ("out", 0), ("share", 2, 0, 0), ("out", 3),
    ("share", 2, 3, 0), ("out", 2), ("share", 2, 2, 0), ("share", 2, 0, 1), ("out", 4),
    ("share", 2, 4, 0), ("share", 2, 3, 1), ("share", 2, 1, 1), ("share", 2, 2, 1),
    ("share", 2, 0, 2), ("share", 2, 0, 3), ("fin", 0), ("share", 2, 4, 1), ("share", 2, 3, 2),
    ("share", 2, 1, 2), ("share", 2, 2, 2), ("share", 2, 3, 3), ("fin", 3), ("share", 2, 4, 2),
    ("share", 2, 1, 3), ("fin", 1), ("share", 2, 2, 3), ("fin", 2), ("share", 2, 4, 3), ("fin", 4),
]


class Program:
    def __init__(self, refs):
        (
            self.tok, self.wu, self.wg, self.wd, *small, self.out,
            self.gain, self.us, self.gs, self.ut, self.gt, self.ds, self.stage, self.scales,
            self.w, self.s, self.x, self.pre, self.halo, self.hid, self.part, self.rd, self.q,
            self.rh, self.rf, self.fin_,
            self.l_sem, self.g_send_sem, self.g_sem, self.i_send_sem, self.i_sem,
            self.s_send_sem, self.s_sem, self.u_send_sem, self.u_sem, self.h_send_sem, self.h_sem,
            self.o_send_sem, self.o_sem, self.know_sem,
        ) = refs
        self.zi, self.yi = lax.axis_index("z"), lax.axis_index("y")
        self.xi, self.ci = lax.axis_index("x"), lax.axis_index("c")
        self.ri = self.zi * NY + self.yi
        self.w_copies = [
            pltpu.make_async_copy((self.wu, self.wg, self.wd)[m % 3].at[m // 3], self.stage.at[m], self.l_sem.at[0])
            for m in range(6)
        ]

        self.small_copies = [
            pltpu.make_async_copy(a, b, self.l_sem.at[2 + k])
            for k, (a, b) in enumerate(
                zip(small, (self.gain, self.us, self.gs, self.ut, self.gt, self.ds), strict=True)
            )
        ]

    def z_of(self, slot):
        return lax.rem(self.zi + offset(slot) + NZ, NZ)

    def enter(self):
        for c in self.w_copies + self.small_copies:
            c.start()
        barrier = pltpu.get_barrier_semaphore()

        def tell(to):
            pl.semaphore_signal(barrier, inc=1, device_id=to, device_id_type=MESH)

        tell(self.step_to("c", "p"))
        for link in "xyz":
            for d in "pm":
                tell(self.step_to(link, d))
        pltpu.make_async_copy(self.stage, self.stage, self.l_sem.at[0]).wait()
        for m in range(6):
            self.w[m, self.ri] = self.stage[m].astype(jnp.bfloat16)
        pl.semaphore_wait(barrier, 7)

    def know(self, k):
        if k > 0:
            pl.semaphore_wait(self.know_sem.at[k - 1], 2)
        if k < 5:
            for d in "pm":
                pl.semaphore_signal(
                    self.know_sem.at[k], inc=1, device_id=self.step_to("y" if k == 0 else "z", d),
                    device_id_type=MESH,
                )

    def gather_region(self, i, key, d, slot):
        m, c0, c1, c2 = ITEMS[i]
        sign = 1 if d == "p" else -1
        hop = int(key[2])
        back = hop - 1
        first, second = pl.ds(c0, c1 - c0), pl.ds(c1, c2 - c1)
        z = lax.rem(self.zi - sign * back + NZ, NZ)
        y = lax.rem(self.yi - sign * back + NY, NY)
        half = pl.ds(0 if d == "p" else 32, 32)
        w = self.w.at[m]
        if key[:2] == "Ay":
            return w.at[self.zi * NY + y, half if hop == 2 else slice(None), first]
        if key[:2] == "Az":
            if hop == 4:
                return w.at[pl.ds(z * NY + (0 if d == "p" else 2), 2), :, first]
            return w.at[pl.ds(z * NY, NY), :, first]
        if key[:2] == "Bz":
            return w.at[z * NY + self.yi, half if hop == 4 else slice(None), second]
        return w.at[self.z_of(slot) * NY + y, half if hop == 2 else slice(None), second]

    def step_to(self, link, d):
        if link == "z":
            return {"z": lax.rem(self.zi + (1 if d == "p" else NZ - 1), NZ)}
        if link == "y":
            return {"y": lax.rem(self.yi + (1 if d == "p" else NY - 1), NY)}
        if link == "x":
            return {"x": lax.rem(self.xi + (1 if d == "p" else NX - 1), NX)}
        return {"c": 1 - self.ci}

    @staticmethod
    def remote(src, dst, send, recv, to):
        return pltpu.make_async_remote_copy(
            src_ref=src, dst_ref=dst, send_sem=send, recv_sem=recv, device_id=to, device_id_type=MESH
        )

    def g_copy(self, i, key, d, slot=None):
        region = self.gather_region(i, key, d, slot)
        k = KEY[key] if slot is None else KEY[key, distance_of(slot)]
        return self.remote(
            region, region, self.g_send_sem.at[0], self.g_sem.at[i, k], self.step_to(key[1], d)
        )

    def g_send(self, i, key, slots=(None,)):
        for slot in slots:
            for d in "pm":
                self.g_copy(i, key, d, slot).start()

    def await_bytes(self, like, sem):
        pltpu.make_async_copy(like, like, sem).wait()

    def g_wait(self, i, key, distance=None):
        m, c0, c1, c2 = ITEMS[i]
        cols = pl.ds(c0, c1 - c0) if key[0] == "A" else pl.ds(c1, c2 - c1)
        shards = {"Ay1": 2, "Ay2": 1, "Az4": 4, "Bz4": 1}.get(key, 8 if key[:2] == "Az" else 2)
        k = KEY[key] if distance is None else KEY[key, distance]
        if distance is not None:
            shards = len(slots_at(distance)) * (2 if key == "By1" else 1)
        self.await_bytes(self.w.at[m, pl.ds(0, shards), :, cols], self.g_sem.at[i, k])

    def g_forward(self, i, came, goes):
        self.g_wait(i, came)
        self.g_send(i, goes)

    def A(self, i, st):
        if st == 0:
            self.g_send(i, "Ay1")
        elif st == 1:
            self.g_forward(i, "Ay1", "Ay2")
        elif st == 2:
            self.g_wait(i, "Ay2")
            self.g_send(i, "Az1")
        elif st < 6:
            self.g_forward(i, f"Az{st - 2}", f"Az{st - 1}")
        else:
            self.g_wait(i, "Az4")

    def B(self, i, st):
        if st == 0:
            self.g_send(i, "Bz1")
        elif st < 4:
            self.g_forward(i, f"Bz{st}", f"Bz{st + 1}")
        else:
            self.g_wait(i, "Bz4")
        self.g_send(i, "By1", slots_at(st))

    def C(self, i, distance):
        self.g_wait(i, "By1", distance)
        self.g_send(i, "By2", slots_at(distance))

    def E(self, i, distance):
        self.g_wait(i, "By2", distance)

    def lanes(self, own=True):
        c = self.ci if own else 1 - self.ci
        return pl.ds(pl.multiple_of(c * 256, 256), 256)

    def rows(self, x):
        return pl.ds(pl.multiple_of(x * 16, 16), 16)

    def in_own(self):
        cols = pl.ds(pl.multiple_of(self.ri * 512 + self.ci * 256, 256), 256)
        rows = pl.ds(pl.multiple_of(self.xi * 16, 16), 16)
        return pltpu.make_async_copy(
            self.tok.at[rows, cols], self.s.at[0, self.ri, self.rows(self.xi), self.lanes()], self.l_sem.at[1]
        )

    def in_copy(self, other):
        cols = pl.ds(pl.multiple_of(other * 512 + self.ci * 256, 256), 256)
        rows = pl.ds(pl.multiple_of(self.xi * 16, 16), 16)
        return self.remote(
            self.tok.at[rows, cols],
            self.s.at[0, self.ri, self.rows(self.xi), self.lanes()],
            self.i_send_sem.at[0],
            self.i_sem.at[0],
            {"z": other // NY, "y": lax.rem(other, NY)},
        )

    def each_other(self, do):
        def body(k, carry):
            do(lax.rem(self.ri + k, NR))
            return carry

        lax.fori_loop(1, NR, body, 0)

    def in_(self, st):
        if st == 0:
            self.in_own().start()
            self.each_other(lambda o: self.in_copy(o).start())
        else:
            self.in_own().wait()
            self.await_bytes(self.fin_.at[pl.ds(0, NR - 1)], self.i_sem.at[0])

    def share_copy(self, which, j, key):
        lo, n = SHARE_CHUNKS[which][j]
        sem = self.s_sem.at[(4 * which + j) * 3 + {"X1": 0, "X2": 1}.get(key[:2], 2)]
        if key[0] == "X":
            sign = 1 if key[2] == "p" else -1
            hop = int(key[1])
            x = lax.rem(self.xi - sign * (hop - 1) + NX, NX)
            if hop == 2:
                n = n // 2
                lo += 0 if key[2] == "p" else n
            to = self.step_to("x", key[2])
        else:
            x = lax.rem(self.xi + {"D0": 0, "D1": NX - 1, "D2": 1, "D3": 2}[key], NX)
            to = self.step_to("c", "p")
        region = self.s.at[which, pl.ds(lo, n), self.rows(x), self.lanes()]
        return self.remote(region, region, self.s_send_sem.at[0], sem, to)

    def share(self, which, j, st):
        lo, n = SHARE_CHUNKS[which][j]
        sem = (4 * which + j) * 3

        def start(*keys):
            for k in keys:
                self.share_copy(which, j, k).start()

        def arrived(quarters, k):
            like = self.s.at[which, pl.ds(lo, n), pl.ds(0, 16 * quarters), self.lanes()]
            self.await_bytes(like, self.s_sem.at[sem + k])

        if st == 0:
            start("X1p", "X1m", "D0")
        elif st == 1:
            arrived(2, 0)
            start("X2p", "X2m", "D1", "D2")
        elif st == 2:
            arrived(1, 1)
            start("D3")
        else:
            arrived(4, 2)

    def prep(self, l):
        def body(k, acc):
            block = self.s[l, pl.ds(k * 4, 4)].reshape(256, 512)
            t = block.T.astype(jnp.float32)
            z = k if l == 0 else self.z_of(k)
            cols = pl.ds(pl.multiple_of(z * 256, 256), 256)
            self.x[:, cols] = (t * self.gain[l : l + 1, cols]).astype(jnp.bfloat16)
            sq = t * t
            return acc + sq[:, :128] + sq[:, 128:]

        acc = lax.fori_loop(0, 8, body, jnp.zeros((512, 128), jnp.float32))
        mean = jnp.sum(acc, axis=1, keepdims=True) * (1.0 / 2048)
        self.inverse = lax.rsqrt(mean + EPS)

    def ug(self, l, n):
        cols = slice(n * 256, n * 256 + 256)
        for k, scale in ((0, self.us), (1, self.gs)):
            w = self.w[3 * l + k, :, :, cols].reshape(2048, 256)
            raw = jnp.dot(self.x[...], w, preferred_element_type=jnp.float32)
            self.pre[k, 8:520, cols] = raw * self.inverse * scale[l : l + 1, cols]

    def halo_copy(self, l, n):
        cols = pl.ds(n * 256, 256)
        wrap = jnp.where(self.yi == NY - 1, 1, 0)
        to = {"z": lax.rem(self.zi + wrap, NZ), "y": lax.rem(self.yi + 1, NY)}
        return self.remote(
            self.pre.at[:, pl.ds(512, 8), cols], self.halo.at[l, :, :, cols],
            self.h_send_sem.at[l], self.h_sem.at[l], to,
        )

    def conv(self, l):
        self.await_bytes(self.halo.at[l], self.h_sem.at[l])
        first = self.ri == 0
        for n in range(6):
            cols = slice(n * 128, n * 128 + 128)
            both = []
            for k, taps in ((0, self.ut), (1, self.gt)):
                before = self.halo[l, k, :, cols]
                self.pre[k, 0:8, cols] = jnp.where(first, jnp.zeros_like(before), before)
                total = taps[0, l : l + 1, cols] * self.pre[k, 6:518, cols]
                total += taps[1, l : l + 1, cols] * self.pre[k, 7:519, cols]
                total += taps[2, l : l + 1, cols] * self.pre[k, 8:520, cols]
                both.append(total)
            up, gate = both
            self.hid[:, cols] = (gate / (1.0 + jnp.exp(-gate)) * up).astype(jnp.bfloat16)
        self.await_bytes(self.halo.at[l], self.h_send_sem.at[l])

    def scale(self):
        def body(k, carry):
            cols = pl.ds(pl.multiple_of(k * 128, 128), 128)
            for l in range(2):
                row = jnp.broadcast_to(self.ds[l : l + 1, cols], (128, 128))
                self.scales[l, pl.ds(k * 2, 2)] = row.T.reshape(2, 4, 16, 128)
            return carry

        lax.fori_loop(0, 16, body, 0)

    def down(self, l, j):
        lo, n = SUM_CHUNKS[l][j]
        width = 2 if n > NY else 1

        def body(k, carry):
            slot = lo // NY + width * k
            w = jnp.concatenate(
                [
                    self.w[3 * l + 2, pl.ds(self.z_of(slot + i) * NY, NY)].reshape(256, 768)
                    for i in range(width)
                ]
            )
            part = lax.dot_general(
                w, self.hid[...], (((1,), (1,)), ((), ())), preferred_element_type=jnp.float32
            ).astype(jnp.bfloat16)
            self.part[l, pl.ds(slot * NY, NY * width)] = part.reshape(NY * width, 4, 16, 512)
            return carry

        lax.fori_loop(0, n // (NY * width), body, 0)

    def sum_copy(self, l, j, key):
        lo, n = SUM_CHUNKS[l][j]
        h = n // 2
        k = (4 * l + j) * 3 + "DAB".index(key[0])
        sems = (self.u_send_sem.at[0], self.u_sem.at[k])
        if key == "D":
            return self.remote(
                self.part.at[l, pl.ds(lo, n), :, :, self.lanes(False)],
                self.rd.at[l, pl.ds(lo, n)], *sems, self.step_to("c", "p"),
            )
        d = key[1]
        if key[0] == "A":
            first = lo + (0 if d == "p" else h)
            return self.remote(
                self.q.at[l, pl.ds(first, h), lax.rem(self.xi + 2, NX)],
                self.rh.at[l, 0 if d == "p" else 1, pl.ds(lo // 2, h)], *sems, self.step_to("x", d),
            )
        return self.remote(
            self.q.at[l, pl.ds(lo, n), lax.rem(self.xi + (1 if d == "p" else NX - 1), NX)],
            self.rf.at[l, 0 if d == "p" else 1, pl.ds(lo, n)], *sems, self.step_to("x", d),
        )

    def sum(self, l, j, st):
        lo, n = SUM_CHUNKS[l][j]
        h = n // 2
        f32, bf16 = jnp.float32, jnp.bfloat16
        rows = pl.ds(lo, n)
        sem = (4 * l + j) * 3
        if st == 0:
            self.sum_copy(l, j, "D").start()
        elif st == 1:
            self.await_bytes(self.rd.at[l, rows], self.u_sem.at[sem])
            mine = self.part[l, rows, :, :, self.lanes()].astype(f32)
            self.q[l, rows] = (mine + self.rd[l, rows].astype(f32)).astype(bf16)
            self.sum_copy(l, j, "Ap").start()
            self.sum_copy(l, j, "Am").start()
        elif st == 2:
            self.await_bytes(self.rh.at[l, :, pl.ds(lo // 2, h)], self.u_sem.at[sem + 1])
            for d, key in ((1, "p"), (-1, "m")):
                x = lax.rem(self.xi + d + NX, NX)
                part = pl.ds(lo + (0 if key == "p" else h), h)
                came = self.rh[l, 0 if key == "p" else 1, pl.ds(lo // 2, h)].astype(f32)
                self.q[l, part, x] = (self.q[l, part, x].astype(f32) + came).astype(bf16)
                self.sum_copy(l, j, "B" + key).start()
        else:
            self.await_bytes(self.rf.at[l, :, rows], self.u_sem.at[sem + 2])
            for slot in range(lo // NY, (lo + n) // NY):
                near, place = pl.ds(slot * NY, NY), pl.ds(self.z_of(slot) * NY, NY)
                total = self.q[l, near, self.xi].astype(f32)
                total += self.rf[l, 0, near].astype(f32) + self.rf[l, 1, near].astype(f32)
                scale = self.scales[l, place, self.xi]
                scale = jnp.concatenate([scale, scale], axis=2)
                old = self.s[l, place if l == 0 else near, self.rows(self.xi), self.lanes()].astype(f32)
                new = (total * scale + RESIDUAL * old).astype(bf16)
                if l == 0:
                    self.s[1, near, self.rows(self.xi), self.lanes()] = new
                else:
                    self.fin_[near] = new
            if l == 1:
                self.each_out(j, lambda slot, y: self.out_copy(slot, y).start())

    def out_copy(self, slot, y):
        return self.remote(
            self.fin_.at[slot * NY + y],
            self.s.at[2, opposite(slot) * NY + self.yi, self.rows(self.xi), self.lanes()],
            self.o_send_sem.at[0],
            self.o_sem.at[distance_of(slot)],
            {"z": self.z_of(slot), "y": y},
        )

    def each_out(self, j, do):
        lo, n = SUM_CHUNKS[1][j]
        for slot in range(lo // NY, (lo + n) // NY):
            for k in range(1 if slot == 0 else 0, NY):
                do(slot, lax.rem(self.yi + k, NY))

    def out_(self, j):
        n = SUM_CHUNKS[1][j][1]
        if j == 0:
            n -= 1
            self.s[2, self.yi, self.rows(self.xi), self.lanes()] = self.fin_[self.yi]
        self.await_bytes(self.fin_.at[pl.ds(0, n)], self.o_sem.at[j])

    def fin(self, j):
        lo, n = SHARE_CHUNKS[2][j]
        for slot in range(lo // NY, (lo + n) // NY):
            self.out[pl.ds(self.z_of(slot) * NY, NY)] = self.s[2, pl.ds(slot * NY, NY)]

    def run(self):
        self.enter()
        for event in ORDER:
            name, rest = event[0], event[1:]
            if self.small_copies and name in ("scale", "prep"):
                for c in self.small_copies:
                    c.wait()
                self.small_copies = []
            if name == "halo":
                self.halo_copy(*rest).start()
            elif name in ("in", "out"):
                getattr(self, name + "_")(*rest)
            else:
                getattr(self, name)(*rest)
        self.await_bytes(self.w.at[:, pl.ds(0, NR - 1)], self.g_send_sem.at[0])
        self.await_bytes(self.fin_.at[pl.ds(0, NR - 1)], self.i_send_sem.at[0])
        self.await_bytes(self.s.at[:, pl.ds(0, 28)], self.s_send_sem.at[0])
        self.await_bytes(self.s.at[pl.ds(0, 2), pl.ds(0, 28)], self.u_send_sem.at[0])
        self.await_bytes(self.fin_.at[pl.ds(0, NR - 1)], self.o_send_sem.at[0])


def kernel(*refs):
    Program(refs).run()


def per_device(
    tokens, norm_gain, up_weight, gate_weight, up_scale, gate_scale, up_taps, gate_taps,
    down_weight, down_scale,
):
    bf16, f32 = jnp.bfloat16, jnp.float32
    hbm = pl.BlockSpec(memory_space=pltpu.HBM)
    dma = pltpu.SemaphoreType.DMA
    n = len(ITEMS)
    arrays = (
        tokens, up_weight, gate_weight, down_weight, norm_gain, up_scale, gate_scale,
        up_taps.transpose(1, 0, 2), gate_taps.transpose(1, 0, 2), down_scale,
    )
    arrays = [pltpu.with_memory_space_constraint(a, pltpu.HBM) for a in arrays]
    out = pl.pallas_call(
        kernel,
        out_shape=jax.ShapeDtypeStruct((NR, 64, 512), bf16),
        in_specs=[hbm] * 10,
        out_specs=pl.BlockSpec(memory_space=pltpu.VMEM),
        scratch_shapes=[
            pltpu.VMEM((2, 2048), f32),
            pltpu.VMEM((2, 768), f32),
            pltpu.VMEM((2, 768), f32),
            pltpu.VMEM((3, 2, 768), f32),
            pltpu.VMEM((3, 2, 768), f32),
            pltpu.VMEM((2, 2048), f32),
            pltpu.VMEM((6, 64, 768), f32),
            pltpu.VMEM((2, NR, 4, 16, 128), f32),
            pltpu.VMEM((6, NR, 64, 768), bf16),
            pltpu.VMEM((3, NR, 64, 512), bf16),
            pltpu.VMEM((512, 2048), bf16),
            pltpu.VMEM((2, 520, 768), f32),
            pltpu.VMEM((2, 2, 8, 768), f32),
            pltpu.VMEM((512, 768), bf16),
            pltpu.VMEM((2, NR, 4, 16, 512), bf16),
            pltpu.VMEM((2, NR, 4, 16, 256), bf16),
            pltpu.VMEM((2, NR, 4, 16, 256), bf16),
            pltpu.VMEM((2, 2, NR // 2, 16, 256), bf16),
            pltpu.VMEM((2, 2, NR, 16, 256), bf16),
            pltpu.VMEM((NR, 16, 256), bf16),
            dma((8,)),
            dma((1,)), dma((n, 20)),
            dma((1,)), dma((1,)),
            dma((1,)), dma((SHARE_SEMS,)),
            dma((1,)), dma((SUM_SEMS,)),
            dma((2,)), dma((2,)),
            dma((1,)), dma((5,)),
            pltpu.SemaphoreType.REGULAR((5,)),
        ],
        compiler_params=pltpu.CompilerParams(
            collective_id=0, has_side_effects=True, vmem_limit_bytes=50 * 2**20
        ),
    )(*arrays)
    return out.transpose(1, 0, 2).reshape(64, NR * 512)


def solution(mesh):
    torus = Mesh(mesh.devices.reshape(NZ, NY, NX, 2), ("z", "y", "x", "c"))
    ra, cb = ("z", "y"), ("x", "c")
    placed = (
        P(ra, None),
        P(),
        P(None, ra, cb),
        P(None, ra, cb),
        P(None, cb),
        P(None, cb),
        P(None, None, cb),
        P(None, None, cb),
        P(None, ra, cb),
        P(),
    )
    return jax.shard_map(
        per_device, mesh=torus, in_specs=placed, out_specs=P(ra, None), check_vma=False
    )
```
